128 devices in a mesh: sp: 16 (over z, y), dp: 8 (over x, core).
Axes of the slice: x: 4, y: 4, z: 4, core: 2. Of those that a mesh axis runs over, the one named last changes fastest.
Arguments:
- residual: bfloat16 [8, 2048, 2048], P('dp', 'sp'), may hold values from -6 to 6
- query: bfloat16 [8, 2048, 1536], P('dp', 'sp'), may hold values from -64 to 64
- latent: bfloat16 [8, 2048, 256], P('dp', 'sp'), may hold values from -6 to 6
- rope_key: bfloat16 [8, 2048, 32], P('dp', 'sp'), may hold values from -64 to 64
- latent_gain: float32 [256], replicated, may hold values from 0.1 to 1.9
- query_gain: float32 [96], replicated, may hold values from 0.7 to 5.6
- key_gain: float32 [96], replicated, may hold values from 0.7 to 5.6
- key_weight: bfloat16 [256, 1024], replicated, may hold values from -0.375 to 0.375
- value_weight: bfloat16 [256, 1024], replicated, may hold values from -0.375 to 0.375
- mix_gain: float32 [1024], replicated, may hold values from 0.1 to 1.9
- out_weight: bfloat16 [1024, 2048], replicated, may hold values from -0.1875 to 0.1875
- ffn_gain: float32 [2048], replicated, may hold values from 0.1 to 1.9
- expert_choice: int32 [8, 2048, 2], P('dp', 'sp'), may hold values from 0 to 127, as said below
- group_prob: float32 [8, 2048], P('dp', 'sp'), may hold values from 0.25 to 1
- expert_prob: float32 [8, 2048, 2], P('dp', 'sp'), may hold values from 0.05 to 1
- gate_weight: bfloat16 [128, 2048, 512], P(('sp', 'dp')), may hold values from -0.125 to 0.125
- up_weight: bfloat16 [128, 2048, 512], P(('sp', 'dp')), may hold values from -0.125 to 0.125
- down_weight: bfloat16 [128, 512, 2048], P(('sp', 'dp')), may hold values from -0.25 to 0.25
Outputs:
- layer_out: bfloat16 [8, 2048, 2048], P('dp', 'sp')
The draws below stay inside these ranges and needn't reach their ends.
Inputs may be any that keep to these rules, and one draw needn't show every extreme that they name: `expert_choice`: A token's two experts differ and lie in one group of 32 consecutive expert numbers. In each aligned block of 128 tokens (the tokens of one device) no expert is named more than 4 times, and every expert of one group is named exactly 4 times in every block.
All inputs are finite; a program needn't handle non-finite values.
Results may differ from the reference program's by a relative error of at most 0.012.
The reference program's roundings to bfloat16 on the way count: a program that leaves them out, or rounds other values in their place, can miss the bound.
Values may be sent and summed in bfloat16 or wider, within the bound.
No kernel may reach another device: no remote copies, remote signals or barrier semaphores. Data moves between devices by JAX's collectives and lax.ppermute only.
A program may use at most 64 MiB of HBM per device.

```python
import jax
import jax.numpy as jnp
from jax import lax

D = 2048
HEADS = 16
NOPE = 64
ROPE = 32
VDIM = 64
LATENT = 256
FF = 512
GROUPS = 4
TOP = 2
SPAN = 64
TOK_DEV = 128
QK = 96
LENGTH = 2048
BATCH = 8
EXPERTS = 128
EPG = 32
CAP = 4
N_SP = 16
N_DP = 8


def paired_rows(key):
    base_key = jax.random.fold_in(key, 11)
    query_key, rope_draw_key = jax.random.split(base_key, 2)
    query_all = jax.random.truncated_normal(query_key, -4.0, 4.0, (BATCH, LENGTH, HEADS, QK), jnp.float32)
    rope_all = jax.random.truncated_normal(rope_draw_key, -4.0, 4.0, (BATCH, LENGTH, ROPE), jnp.float32)
    return (query_all.reshape(BATCH, LENGTH, HEADS * QK), rope_all)


def draw_query(key, part):
    return paired_rows(key)[0].astype(jnp.bfloat16)


def draw_rope_key(key, part):
    return paired_rows(key)[1].astype(jnp.bfloat16)


def head_gains(key, salt):
    gain_key = jax.random.fold_in(key, salt)
    gains = jax.random.uniform(gain_key, (QK,), jnp.float32, 0.7, 1.3)
    return gains


def draw_query_gain(key, part):
    return head_gains(key, 21)


def draw_key_gain(key, part):
    return head_gains(key, 22)


def draw_expert_choice(key, part):
    base_key = jax.random.fold_in(key, 31)
    hot_key, block_key = jax.random.split(base_key)
    half_rows = TOK_DEV // 2
    block_total = BATCH * LENGTH // TOK_DEV
    hot_group = jax.random.randint(hot_key, (), 0, GROUPS)

    def one_block(sub_key):
        cut_key, offset_key, shift_key, order_key = jax.random.split(sub_key, 4)
        cuts = jnp.sort(jax.random.randint(cut_key, (2,), 0, half_rows + 1))
        position = jnp.arange(TOK_DEV, dtype=jnp.int32)
        rest_pos = position - half_rows
        other_index = (rest_pos >= cuts[0]).astype(jnp.int32) + (rest_pos >= cuts[1]).astype(jnp.int32)
        other_group = (hot_group + 1 + other_index) % GROUPS
        group_of = jnp.where(position < half_rows, hot_group, other_group)
        other_start = jnp.where(other_index == 0, half_rows, jnp.where(other_index == 1, half_rows + cuts[0], half_rows + cuts[1]))
        group_start = jnp.where(position < half_rows, 0, other_start)
        rank_in = position - group_start
        offsets = jax.random.randint(offset_key, (GROUPS,), 0, EPG)
        shifts = jax.random.randint(shift_key, (GROUPS,), 1, EPG)
        first_local = (rank_in + offsets[group_of]) % EPG
        second_local = (first_local + shifts[group_of]) % EPG
        pairs = jnp.stack([group_of * EPG + first_local, group_of * EPG + second_local], axis=-1)
        shuffle = jax.random.permutation(order_key, TOK_DEV)
        return pairs[shuffle]
    blocks = jax.vmap(one_block)(jax.random.split(block_key, block_total))
    return blocks.reshape(BATCH, LENGTH, TOP).astype(jnp.int32)


def shard_levels(rng, shape, cuts, smallest, largest):
    gain = 1.0
    for dim, shards_of in cuts:
        heights = jax.random.uniform(jax.random.fold_in(jax.random.fold_in(rng, 6), dim), (shards_of,), jnp.float32, smallest / len(cuts), largest / len(cuts))
        gain = gain * jnp.repeat(jnp.exp(heights), shape[dim] // shards_of).reshape((-1,) + (1,) * (len(shape) - 1 - dim))
    return gain


def noise(stream_key, shape, width, bound, shards=(), kind=jnp.bfloat16):
    values = width * jax.random.normal(stream_key, shape, jnp.float32)
    if shards:
        values = values * shard_levels(stream_key, shape, shards, -0.22, 0.18)
    return jnp.clip(values, -bound, bound).astype(kind)


def setup_inputs(seed: int = 0) -> dict:
    key_list = jax.random.split(jax.random.key(seed), 19)
    return {
        "residual": noise(key_list[0], (BATCH, LENGTH, D), 1.0, 6.0, ((0, 8), (1, 16))),
        "query": draw_query(jax.random.fold_in(key_list[18], 71), 0),
        "latent": noise(key_list[2], (BATCH, LENGTH, LATENT), 1.0, 6.0, ((0, 8), (1, 16))),
        "rope_key": draw_rope_key(jax.random.fold_in(key_list[18], 71), 0),
        "latent_gain": jnp.clip(1.0 + 0.18 * jax.random.normal(key_list[4], (LATENT,), jnp.float32), 0.1, 1.9),
        "query_gain": draw_query_gain(jax.random.fold_in(key_list[18], 71), 0),
        "key_gain": draw_key_gain(jax.random.fold_in(key_list[18], 71), 0),
        "key_weight": noise(key_list[7], (LATENT, HEADS * NOPE), LATENT ** -0.5, 0.375),
        "value_weight": noise(key_list[8], (LATENT, HEADS * VDIM), LATENT ** -0.5, 0.375),
        "mix_gain": jnp.clip(1.0 + 0.18 * jax.random.normal(key_list[9], (HEADS * VDIM,), jnp.float32), 0.1, 1.9),
        "out_weight": noise(key_list[10], (HEADS * VDIM, D), (HEADS * VDIM) ** -0.5, 0.1875),
        "ffn_gain": jnp.clip(1.0 + 0.18 * jax.random.normal(key_list[11], (D,), jnp.float32), 0.1, 1.9),
        "expert_choice": draw_expert_choice(jax.random.fold_in(key_list[18], 71), 0),
        "group_prob": jnp.clip(0.25 + 0.75 * jax.random.uniform(key_list[13], (BATCH, LENGTH), jnp.float32) ** shard_levels(key_list[13], (BATCH, LENGTH), ((0, 8), (1, 16)), -0.2, 0.2), 0.25, 1.0),
        "expert_prob": jnp.clip(0.05 + 0.95 * jax.random.uniform(key_list[14], (BATCH, LENGTH, TOP), jnp.float32) ** shard_levels(key_list[14], (BATCH, LENGTH, TOP), ((0, 8), (1, 16)), -0.2, 0.2), 0.05, 1.0),
        "gate_weight": noise(key_list[15], (EXPERTS, D, FF), D ** -0.5, 0.125, ((0, 128),)),
        "up_weight": noise(key_list[16], (EXPERTS, D, FF), D ** -0.5, 0.125, ((0, 128),)),
        "down_weight": noise(key_list[17], (EXPERTS, FF, D), FF ** -0.5, 0.25, ((0, 128),)),
    }


eps = 1e-06

def rms_scale(vector, gains):
    return vector * lax.rsqrt(lax.optimization_barrier(jnp.mean(vector * vector, axis=-1, keepdims=True)) + eps) * gains

def rotate(vector, phases):
    half_width = vector.shape[-1] // 2
    lower_half = vector[..., :half_width]
    upper_half = vector[..., half_width:]
    cos_table = jnp.cos(phases)
    sin_table = jnp.sin(phases)
    return jnp.concatenate([lower_half * cos_table - upper_half * sin_table, upper_half * cos_table + lower_half * sin_table], axis=-1)

def angles(offset, span_count, rope_width):
    position = (offset + jnp.arange(span_count, dtype=jnp.int32)).astype(jnp.float32)
    frequency = 10000.0 ** (-2.0 * jnp.arange(rope_width // 2, dtype=jnp.float32) / rope_width)
    return position[:, None] * frequency[None, :]

def head_vectors(nope_part, rope_part, gains, phases):
    normed_all = rms_scale(jnp.concatenate([nope_part, rope_part], axis=-1), gains)
    split_at = nope_part.shape[-1]
    turned = rotate(normed_all[..., split_at:], phases[:, None, :])
    return jnp.concatenate([normed_all[..., :split_at], turned], axis=-1).astype(jnp.bfloat16)

def attend_one(query_head, key_head, value_head):
    length = query_head.shape[0]
    blocks_count = max(4, length // 1024)
    block_rows = length // blocks_count
    score_scale = query_head.shape[-1] ** (-0.5)
    pieces = []
    for block_index in range(blocks_count):
        first_row = block_index * block_rows
        last_row = first_row + block_rows
        scores = jnp.dot(query_head[first_row:last_row], key_head[:last_row].T, preferred_element_type=jnp.float32) * score_scale
        query_pos = first_row + jnp.arange(block_rows, dtype=jnp.int32)
        key_pos = jnp.arange(last_row, dtype=jnp.int32)
        allowed = key_pos[None, :] // SPAN <= query_pos[:, None] // SPAN
        scores = jnp.where(allowed, scores, -1e+30)
        row_top = lax.optimization_barrier(jnp.max(scores, axis=-1, keepdims=True))
        raised = jnp.exp(scores - row_top)
        row_sum = lax.optimization_barrier(jnp.sum(raised, axis=-1))
        summed = jnp.dot(raised.astype(jnp.bfloat16), value_head[:last_row], preferred_element_type=jnp.float32)
        pieces.append((summed / row_sum[:, None]).astype(jnp.bfloat16))
    return jnp.concatenate(pieces, axis=0)

def reference(residual, query, latent, rope_key, latent_gain, query_gain, key_gain, key_weight, value_weight, mix_gain, out_weight, ffn_gain, expert_choice, group_prob, expert_prob, gate_weight, up_weight, down_weight):
    phases = angles(0, LENGTH, ROPE)
    raw_query = query.astype(jnp.float32).reshape(BATCH, LENGTH, HEADS, QK)
    queries = head_vectors(raw_query[..., :NOPE], raw_query[..., NOPE:], query_gain, phases)
    normed_latent = rms_scale(latent.astype(jnp.float32), latent_gain).astype(jnp.bfloat16)
    flat_latent = normed_latent.reshape(BATCH * LENGTH, LATENT)
    key_part = jnp.dot(flat_latent, key_weight, preferred_element_type=jnp.float32).astype(jnp.bfloat16)
    key_part = key_part.reshape(BATCH, LENGTH, HEADS, NOPE)
    values = jnp.dot(flat_latent, value_weight, preferred_element_type=jnp.float32).astype(jnp.bfloat16)
    values = values.reshape(BATCH, LENGTH, HEADS, VDIM)
    shared_rope = jnp.broadcast_to(rope_key.astype(jnp.float32)[:, :, None, :], (BATCH, LENGTH, HEADS, ROPE))
    keys = head_vectors(key_part.astype(jnp.float32), shared_rope, key_gain, phases)

    def arrange(array):
        return array.transpose(0, 2, 1, 3).reshape(BATCH * HEADS, LENGTH, array.shape[-1])

    def per_head(operands):
        return attend_one(operands[0], operands[1], operands[2])
    heads_out = lax.map(per_head, (arrange(queries), arrange(keys), arrange(values)))
    heads_out = heads_out.reshape(BATCH, HEADS, LENGTH, VDIM).transpose(0, 2, 1, 3).reshape(BATCH * LENGTH, HEADS * VDIM)
    mixed_in = rms_scale(heads_out.astype(jnp.float32), mix_gain).astype(jnp.bfloat16)
    stream = residual.reshape(BATCH * LENGTH, D).astype(jnp.float32) + jnp.dot(mixed_in, out_weight, preferred_element_type=jnp.float32)
    normed = rms_scale(stream, ffn_gain).astype(jnp.bfloat16)
    shares = expert_prob.reshape(BATCH * LENGTH, TOP)
    route_weight = group_prob.reshape(BATCH * LENGTH, 1) * shares / lax.optimization_barrier(jnp.sum(shares, axis=-1, keepdims=True))
    flat_choice = expert_choice.reshape(BATCH * LENGTH * TOP)
    flat_route = route_weight.reshape(BATCH * LENGTH * TOP)
    assignments = BATCH * LENGTH * TOP
    most_rows = CAP * N_SP * N_DP

    def serve_expert(running, operands):
        expert_id, gate_one, up_one, down_one = operands
        picked = jnp.nonzero(flat_choice == expert_id, size=most_rows, fill_value=assignments)[0].astype(jnp.int32)
        token_ids = picked // TOP
        rows_in = jnp.take(normed, token_ids, axis=0, mode='fill', fill_value=0)
        gate_act = jnp.dot(rows_in, gate_one, preferred_element_type=jnp.float32)
        upward = jnp.dot(rows_in, up_one, preferred_element_type=jnp.float32)
        hidden = (jax.nn.silu(gate_act) * upward).astype(jnp.bfloat16)
        expert_out = jnp.dot(hidden, down_one, preferred_element_type=jnp.float32).astype(jnp.bfloat16)
        weight_of = jnp.take(flat_route, picked, mode='fill', fill_value=0.0)
        running = running.at[token_ids].add(weight_of[:, None] * expert_out.astype(jnp.float32), mode='drop')
        return (running, None)
    start_sum = jnp.zeros((BATCH * LENGTH, D), jnp.float32)
    routed_sum, _ = lax.scan(serve_expert, start_sum, (jnp.arange(EXPERTS, dtype=jnp.int32), gate_weight, up_weight, down_weight))
    return (stream + routed_sum).astype(jnp.bfloat16).reshape(BATCH, LENGTH, D)
```

```python
import jax
import jax.numpy as jnp
from jax import lax
from jax.experimental import pallas as pl
from jax.experimental.pallas import tpu as pltpu
from jax.sharding import PartitionSpec as P

SPAN = 64
LANES = 128
SLOTS = 4

eps = 1e-06


def angles(offset, span_count, rope_width):
    position = (offset + jnp.arange(span_count, dtype=jnp.int32)).astype(jnp.float32)
    frequency = 10000.0 ** (-2.0 * jnp.arange(rope_width // 2, dtype=jnp.float32) / rope_width)
    return position[:, None] * frequency[None, :]


def lane_iota(rows, width=LANES):
    return lax.broadcasted_iota(jnp.int32, (rows, width), 1)


def inverse_rms(vector, width):
    return lax.rsqrt(jnp.sum(vector * vector, axis=-1, keepdims=True) * (1.0 / width) + eps)


def project_kernel(query, latent, rope, latent_gain, gains, turn, key_weight, value_weight, out):
    rows = query.shape[0]
    heads = query.shape[1] // 96
    lane = lane_iota(rows)
    raw_latent = latent[...].astype(jnp.float32)
    normed_latent = (
        raw_latent * inverse_rms(raw_latent, raw_latent.shape[1]) * latent_gain[...]
    ).astype(jnp.bfloat16)
    key_part = (
        jnp.dot(normed_latent, key_weight[...], preferred_element_type=jnp.float32)
        .astype(jnp.bfloat16)
        .astype(jnp.float32)
    )
    values = jnp.dot(normed_latent, value_weight[...], preferred_element_type=jnp.float32)
    place = (
        lax.broadcasted_iota(jnp.int32, (32, LANES), 0) + 64 == lane_iota(32)
    ).astype(jnp.bfloat16)
    rope_part = jnp.dot(rope[...], place, preferred_element_type=jnp.float32)
    cos_part = turn[:, 0:128]
    minus_sin = turn[:, 128:256]
    plus_sin = turn[:, 256:384]

    def finish(vector, gain):
        scaled = vector * inverse_rms(vector, 96) * gain
        return (
            scaled * cos_part
            + pltpu.roll(scaled, 112, 1) * minus_sin
            + pltpu.roll(scaled, 16, 1) * plus_sin
        )

    for head in range(heads):
        first = head * 96
        tile, shift = first // 128, first % 128
        here = query[:, tile * 128 : tile * 128 + 128].astype(jnp.float32)
        if shift:
            here = pltpu.roll(here, 128 - shift, 1)
        if shift > 32:
            after = query[:, tile * 128 + 128 : tile * 128 + 256].astype(jnp.float32)
            here = jnp.where(lane < 128 - shift, here, pltpu.roll(after, 128 - shift, 1))
        raw_query = jnp.where(lane < 96, here, 0.0)
        pair = (head // 2) * 128
        raw_key = key_part[:, pair : pair + 128]
        value = values[:, pair : pair + 128]
        if head % 2:
            raw_key = pltpu.roll(raw_key, 64, 1)
            value_first, value_second = pltpu.roll(value, 32, 1), value
        else:
            value_first, value_second = pltpu.roll(value, 96, 1), pltpu.roll(value, 64, 1)
        raw_key = jnp.where(lane < 64, raw_key, rope_part)
        head_query = finish(raw_query, gains[0:1, :])
        head_key = finish(raw_key, gains[1:2, :])
        span = slice(head * rows, (head + 1) * rows)
        out[span, 0:128] = jnp.where(lane < 96, head_query, value_first).astype(jnp.bfloat16)
        out[span, 128:256] = jnp.where(lane < 96, head_key, value_second).astype(jnp.bfloat16)


def attend_kernel(packed, out):
    length = packed.shape[0]
    rows = 256
    scale = 96 ** (-0.5)
    keep = (lane_iota(rows) < 96).astype(jnp.bfloat16)
    query_seg = lax.broadcasted_iota(jnp.int32, (rows, rows), 0) // SPAN
    key_seg = lax.broadcasted_iota(jnp.int32, (rows, rows), 1) // SPAN
    allowed = key_seg <= query_seg
    lane = lane_iota(64)
    for block in range(length // rows):
        first, last = block * rows, (block + 1) * rows
        head_query = packed[first:last, 0:128] * keep
        own = lax.dot_general(
            head_query,
            packed[first:last, 128:256],
            (((1,), (1,)), ((), ())),
            preferred_element_type=jnp.float32,
        )
        own = jnp.where(allowed, own, -1e30)
        top = jnp.max(own, axis=-1, keepdims=True)
        if block:
            past = lax.dot_general(
                head_query,
                packed[0:first, 128:256],
                (((1,), (1,)), ((), ())),
                preferred_element_type=jnp.float32,
            )
            top = jnp.maximum(top, jnp.max(past, axis=-1, keepdims=True))
        raised = jnp.exp((own - top) * scale)
        row_sum = jnp.sum(raised, axis=-1, keepdims=True)
        summed = jnp.dot(
            raised.astype(jnp.bfloat16), packed[first:last, :], preferred_element_type=jnp.float32
        )
        if block:
            raised = jnp.exp((past - top) * scale)
            row_sum = row_sum + jnp.sum(raised, axis=-1, keepdims=True)
            summed = summed + jnp.dot(
                raised.astype(jnp.bfloat16), packed[0:first, :], preferred_element_type=jnp.float32
            )
        summed = summed / row_sum
        for half in range(2):
            low = summed[half * 128 : half * 128 + 64]
            high = summed[half * 128 + 64 : half * 128 + 128]
            joined = jnp.where(
                lane < 64,
                jnp.where(lane < 32, pltpu.roll(low[:, :128], 32, 1), pltpu.roll(low[:, 128:], 64, 1)),
                jnp.where(lane < 96, pltpu.roll(high[:, :128], 96, 1), high[:, 128:]),
            )
            at = (block * 2 + half) * 64
            out[at : at + 64, :] = joined.astype(jnp.bfloat16)


def route_kernel(choice, spread, gather):
    tokens = choice.shape[0]
    experts = lane_iota(tokens)
    first = choice[:, 0:1]
    second = choice[:, 1:2]
    hot_first = (first == experts).astype(jnp.float32)
    hot_second = (second == experts).astype(jnp.float32)
    earlier = (
        lane_iota(tokens) < lax.broadcasted_iota(jnp.int32, (tokens, LANES), 0)
    ).astype(jnp.bfloat16)
    count_first = jnp.dot(
        earlier, hot_first.astype(jnp.bfloat16), preferred_element_type=jnp.float32
    )
    count_second = jnp.dot(
        earlier, hot_second.astype(jnp.bfloat16), preferred_element_type=jnp.float32
    ) + jnp.sum(hot_first, axis=0, keepdims=True)
    rank_first = jnp.sum(count_first * hot_first, axis=-1, keepdims=True).astype(jnp.int32)
    rank_second = jnp.sum(count_second * hot_second, axis=-1, keepdims=True).astype(jnp.int32)
    wide = lane_iota(tokens, 512)
    gather[0:tokens, :] = (first * SLOTS + rank_first == wide).astype(jnp.float32).astype(jnp.bfloat16)
    gather[tokens : 2 * tokens, :] = (
        (second * SLOTS + rank_second == wide).astype(jnp.float32).astype(jnp.bfloat16)
    )
    row_first = jnp.broadcast_to((first * 8 + rank_first).astype(jnp.float32), (tokens, LANES))
    row_second = jnp.broadcast_to((second * 8 + rank_second).astype(jnp.float32), (tokens, LANES))
    row_first = row_first.T[0:1, :].astype(jnp.int32)
    row_second = row_second.T[0:1, :].astype(jnp.int32)
    slot_row = lax.broadcasted_iota(jnp.int32, (spread.shape[0], LANES), 0)
    for half in range(2):
        picked = (slot_row == row_first + 4 * half) | (slot_row == row_second + 4 * half)
        spread[:, half * 128 : half * 128 + 128] = picked.astype(jnp.float32).astype(jnp.bfloat16)


def mix_kernel(
    arrived, residual, mix_gain, out_weight, ffn_gain, spread, stream_out, outgoing, heads_out
):
    tokens = residual.shape[0]
    half_rows = tokens // 2
    lane = lane_iota(half_rows)
    width = residual.shape[1]
    square_low = jnp.zeros((half_rows, 1), jnp.float32)
    square_high = jnp.zeros((half_rows, 1), jnp.float32)
    pairs = arrived.shape[0] // tokens
    for pair in range(pairs):
        one = arrived[pair * tokens : pair * tokens + half_rows, :].astype(jnp.float32)
        two = arrived[pair * tokens + half_rows : (pair + 1) * tokens, :].astype(jnp.float32)
        low = jnp.where(lane < 64, one, pltpu.roll(two, 64, 1))
        high = jnp.where(lane < 64, pltpu.roll(one, 64, 1), two)
        square_low = square_low + jnp.sum(low * low, axis=-1, keepdims=True)
        square_high = square_high + jnp.sum(high * high, axis=-1, keepdims=True)
        heads_out[0:half_rows, pair * 128 : pair * 128 + 128] = low
        heads_out[half_rows:tokens, pair * 128 : pair * 128 + 128] = high
    squares = jnp.concatenate([square_low, square_high], axis=0)
    inverse = lax.rsqrt(squares * (1.0 / heads_out.shape[1]) + eps)
    mixed_in = (heads_out[...] * inverse * mix_gain[...]).astype(jnp.bfloat16)
    stream = residual[...].astype(jnp.float32) + jnp.dot(
        mixed_in, out_weight[...], preferred_element_type=jnp.float32
    )
    stream_out[...] = stream
    normed = (stream * inverse_rms(stream, width) * ffn_gain[...]).astype(jnp.bfloat16)
    stacked = jnp.concatenate([normed[:, : width // 2], normed[:, width // 2 :]], axis=0)
    outgoing[...] = jnp.dot(
        spread[...], stacked, preferred_element_type=jnp.float32
    ).astype(jnp.bfloat16)


def unstack(blocks, rows_out):
    pairs, width = blocks.shape[0] // 16, blocks.shape[1]
    view = blocks[...].astype(jnp.float32).reshape(pairs, 2, 8, width)
    one, two = view[:, 0], view[:, 1]
    upper = lax.broadcasted_iota(jnp.int32, (pairs, 8, width), 1) < 4
    low = jnp.where(upper, one, pltpu.roll(two, 4, 1))
    high = jnp.where(upper, pltpu.roll(one, 4, 1), two)
    rows_out[:, 0:width] = low.reshape(pairs * 8, width).astype(jnp.bfloat16)
    rows_out[:, width : 2 * width] = high.reshape(pairs * 8, width).astype(jnp.bfloat16)


def expert_kernel(arrived, gate_weight, up_weight, down_weight, out, rows_in):
    unstack(arrived, rows_in)
    gate_act = jnp.dot(rows_in[...], gate_weight[0], preferred_element_type=jnp.float32)
    upward = jnp.dot(rows_in[...], up_weight[0], preferred_element_type=jnp.float32)
    hidden = (jax.nn.silu(gate_act) * upward).astype(jnp.bfloat16)
    expert_out = jnp.dot(hidden, down_weight[0], preferred_element_type=jnp.float32)
    rows, width = expert_out.shape
    width = width // 2
    low = expert_out[:, :width].reshape(rows // 8, 8, width)
    high = expert_out[:, width:].reshape(rows // 8, 8, width)
    upper = lax.broadcasted_iota(jnp.int32, (rows // 8, 8, width), 1) < 4
    one = jnp.where(upper, low, pltpu.roll(high, 4, 1))
    two = jnp.where(upper, pltpu.roll(low, 4, 1), high)
    both = jnp.concatenate([one[:, None], two[:, None]], axis=1)
    out[...] = both.reshape(rows * 2, width).astype(jnp.bfloat16)


def combine_kernel(returned, gather, stream, route_weight, out, rows_back):
    unstack(returned, rows_back)
    tokens = stream.shape[0]
    picked = jnp.dot(gather[...], rows_back[...], preferred_element_type=jnp.float32)
    routed = route_weight[:, 0:1] * picked[:tokens] + route_weight[:, 1:2] * picked[tokens:]
    out[...] = (stream[...] + routed).astype(jnp.bfloat16)


def call(body, out_shapes, scratch=(), name=None):
    return pl.pallas_call(
        body,
        out_shape=out_shapes,
        scratch_shapes=list(scratch),
        compiler_params=pltpu.CompilerParams(vmem_limit_bytes=56 * 2**20),
        name=name,
    )


def per_device(
    residual,
    query,
    latent,
    rope_key,
    latent_gain,
    query_gain,
    key_gain,
    key_weight,
    value_weight,
    mix_gain,
    out_weight,
    ffn_gain,
    expert_choice,
    group_prob,
    expert_prob,
    gate_weight,
    up_weight,
    down_weight,
):
    tokens = residual.shape[1]
    width = residual.shape[2]
    sequence = tokens * lax.axis_size("sp")
    shape = jax.ShapeDtypeStruct
    phases = angles(lax.axis_index("sp") * tokens, tokens, rope_key.shape[2])
    cos_table, sin_table = jnp.cos(phases), jnp.sin(phases)
    ones, none = jnp.ones((tokens, 64), jnp.float32), jnp.zeros((tokens, 64), jnp.float32)
    turn = jnp.concatenate(
        [
            ones,
            cos_table,
            cos_table,
            none[:, :32],
            none,
            -sin_table,
            none[:, :48],
            none,
            none[:, :16],
            sin_table,
            none[:, :32],
        ],
        axis=1,
    )
    gains = jnp.pad(jnp.stack([query_gain, key_gain]), ((0, 0), (0, 32)))
    packed = call(project_kernel, shape((16 * tokens, 256), jnp.bfloat16), name="project")(
        query[0],
        latent[0],
        rope_key[0],
        latent_gain[None],
        gains,
        turn,
        key_weight,
        value_weight,
    )
    by_head = lax.all_to_all(packed, "sp", split_axis=0, concat_axis=0, tiled=True)
    spread, gather = call(
        route_kernel,
        (shape((1024, 256), jnp.bfloat16), shape((256, 512), jnp.bfloat16)),
        name="route",
    )(expert_choice[0])
    expert_share = expert_prob[0]
    route_weight = (
        group_prob[0][:, None] * expert_share / jnp.sum(expert_share, axis=-1, keepdims=True)
    )
    head_out = call(attend_kernel, shape((sequence // 2, 128), jnp.bfloat16), name="attend")(by_head)
    by_token = lax.all_to_all(head_out, "sp", split_axis=0, concat_axis=0, tiled=True)
    stream, outgoing = call(
        mix_kernel,
        (shape((tokens, width), jnp.float32), shape((1024, 1024), jnp.bfloat16)),
        scratch=(pltpu.VMEM((tokens, 1024), jnp.float32),),
        name="mix",
    )(by_token, residual[0], mix_gain[None], out_weight, ffn_gain[None], spread)
    arrived = lax.all_to_all(outgoing, ("sp", "dp"), split_axis=0, concat_axis=0, tiled=True)
    answers = call(
        expert_kernel,
        shape((1024, 1024), jnp.bfloat16),
        scratch=(pltpu.VMEM((512, width), jnp.bfloat16),),
        name="expert",
    )(arrived, gate_weight, up_weight, down_weight)
    returned = lax.all_to_all(answers, ("sp", "dp"), split_axis=0, concat_axis=0, tiled=True)
    return call(
        combine_kernel,
        shape((tokens, width), jnp.bfloat16),
        scratch=(pltpu.VMEM((512, width), jnp.bfloat16),),
        name="combine",
    )(returned, gather, stream, route_weight)[None]


def solution(mesh):
    return jax.shard_map(
        per_device,
        mesh=mesh,
        in_specs=(
            P("dp", "sp", None),
            P("dp", "sp", None),
            P("dp", "sp", None),
            P("dp", "sp", None),
            P(),
            P(),
            P(),
            P(),
            P(),
            P(),
            P(),
            P(),
            P("dp", "sp", None),
            P("dp", "sp"),
            P("dp", "sp", None),
            P(("sp", "dp"), None, None),
            P(("sp", "dp"), None, None),
            P(("sp", "dp"), None, None),
        ),
        out_specs=P("dp", "sp", None),
        check_vma=False,
    )
```

```python
import jax
import jax.numpy as jnp
from jax import lax
from jax.experimental import pallas as pl
from jax.experimental.pallas import tpu as pltpu
from jax.sharding import PartitionSpec as P

SPAN = 64
LANES = 128
SLOTS = 4

eps = 1e-06


def angles(offset, span_count, rope_width):
    position = (offset + jnp.arange(span_count, dtype=jnp.int32)).astype(jnp.float32)
    frequency = 10000.0 ** (-2.0 * jnp.arange(rope_width // 2, dtype=jnp.float32) / rope_width)
    return position[:, None] * frequency[None, :]


def lane_iota(rows, width=LANES):
    return lax.broadcasted_iota(jnp.int32, (rows, width), 1)


def inverse_rms(vector, width):
    return lax.rsqrt(jnp.sum(vector * vector, axis=-1, keepdims=True) * (1.0 / width) + eps)


def turn_lanes(vector, cos_part, minus_sin, plus_sin):
    return (
        vector * cos_part
        + pltpu.roll(vector, 112, 1) * minus_sin
        + pltpu.roll(vector, 16, 1) * plus_sin
    )


def split_high_low(vector):
    high = vector.astype(jnp.bfloat16)
    low = (vector - high.astype(jnp.float32)).astype(jnp.bfloat16)
    return jnp.concatenate([high, low], axis=1)


def same_group(group_of_row, group_of_lane):
    ones = (group_of_row == group_of_lane).astype(jnp.float32).astype(jnp.bfloat16)
    return jnp.concatenate([ones, ones], axis=0)


def project_kernel(
    query,
    latent,
    rope,
    latent_gain,
    query_gain,
    key_gain,
    cos_table,
    sin_table,
    key_weight,
    value_weight,
    out,
    small,
    turn,
):
    rows = query.shape[0]
    heads = query.shape[1] // 96
    lane = lane_iota(rows)
    raw_latent = latent[...].astype(jnp.float32)
    normed_latent = (
        raw_latent * inverse_rms(raw_latent, raw_latent.shape[1]) * latent_gain[...]
    ).astype(jnp.bfloat16)
    key_part = (
        jnp.dot(normed_latent, key_weight[...], preferred_element_type=jnp.float32)
        .astype(jnp.bfloat16)
        .astype(jnp.float32)
    )
    values = jnp.dot(normed_latent, value_weight[...], preferred_element_type=jnp.float32)

    small[...] = jnp.zeros(small.shape, jnp.float32)
    small[0:1, 0:96] = query_gain[...]
    small[8:9, 0:96] = key_gain[...]
    turn[:, 0:128] = jnp.ones((rows, 128), jnp.float32)
    turn[:, 128:384] = jnp.zeros((rows, 256), jnp.float32)
    turn[:, 64:80] = cos_table[...]
    turn[:, 80:96] = cos_table[...]
    turn[:, 192:208] = -sin_table[...]
    turn[:, 336:352] = sin_table[...]
    tables = [turn[:, 0:128], turn[:, 128:256], turn[:, 256:384]]
    gain_row = small[0:8, :]
    key_gain_row = small[8:9, :]
    gain_tiles = [
        (gain_row + pltpu.roll(gain_row, 96, 1) * (lane_iota(8) >= 96).astype(jnp.float32))[0:1],
        jnp.where(lane_iota(8) < 64, pltpu.roll(gain_row, 96, 1), pltpu.roll(gain_row, 64, 1))[0:1],
        jnp.where(lane_iota(8) < 32, pltpu.roll(gain_row, 64, 1), pltpu.roll(gain_row, 32, 1))[0:1],
    ]
    turn_tiles = [
        tables,
        [pltpu.roll(t, 96, 1) for t in tables],
        [jnp.where(lane < 64, pltpu.roll(t, 64, 1), pltpu.roll(t, 32, 1)) for t in tables],
    ]
    wide_row = lax.broadcasted_iota(jnp.int32, (128, 256), 0)
    wide_lane = lax.broadcasted_iota(jnp.int32, (128, 256), 1)
    sum_low = same_group(wide_row // 96, wide_lane // 96)
    sum_mid = same_group((wide_row + 128) // 96, wide_lane // 96)
    sum_mid_last = same_group(
        (lax.broadcasted_iota(jnp.int32, (128, 128), 0) + 128) // 96, (lane_iota(128) + 256) // 96
    )
    sum_high = same_group((wide_row + 256) // 96, (wide_lane + 128) // 96)
    sum_pair = same_group(
        lax.broadcasted_iota(jnp.int32, (128, 128), 0) // 64, lane_iota(128) // 64
    )
    sum_all = jnp.ones((256, 128), jnp.bfloat16)

    place = (
        lax.broadcasted_iota(jnp.int32, (32, LANES), 0) + 64 == lane_iota(32)
    ).astype(jnp.float32).astype(jnp.bfloat16)
    rope_part = lax.dot_general(
        rope[...], place, (((0,), (0,)), ((), ())), preferred_element_type=jnp.float32
    )
    rope_square = jnp.dot(
        split_high_low(rope_part * rope_part), sum_all, preferred_element_type=jnp.float32
    )
    rope_turned = turn_lanes(rope_part * key_gain_row, *tables)
    rope_at = [rope_turned] + [pltpu.roll(rope_turned, shift, 1) for shift in (96, 64, 32)]
    low_gain = jnp.where(lane_iota(8) < 64, small[8:16, :], pltpu.roll(small[8:16, :], 64, 1))[0:1]

    for four in range(heads // 4):
        raw = [
            query[:, four * 384 + t * 128 : four * 384 + t * 128 + 128].astype(jnp.float32)
            for t in range(3)
        ]
        squares = [split_high_low(t * t) for t in raw]
        from_low = jnp.dot(squares[0], sum_low, preferred_element_type=jnp.float32)
        from_mid = jnp.dot(squares[1], sum_mid, preferred_element_type=jnp.float32)
        from_mid_last = jnp.dot(squares[1], sum_mid_last, preferred_element_type=jnp.float32)
        from_high = jnp.dot(squares[2], sum_high, preferred_element_type=jnp.float32)
        sums = [
            from_low[:, :128] + from_mid[:, :128],
            from_low[:, 128:] + from_mid[:, 128:] + from_high[:, :128],
            from_mid_last + from_high[:, 128:],
        ]
        turned = [
            turn_lanes(
                raw[t] * lax.rsqrt(sums[t] * (1.0 / 96) + eps) * gain_tiles[t], *turn_tiles[t]
            )
            for t in range(3)
        ]
        query_at = [
            turned[0],
            jnp.where(lane < 96, turned[1], turned[0]),
            jnp.where(lane < 64, turned[2], turned[1]),
            turned[2],
        ]
        for pair in range(2):
            at = (four * 2 + pair) * 128
            part = key_part[:, at : at + 128]
            value = values[:, at : at + 128]
            sums = (
                jnp.dot(split_high_low(part * part), sum_pair, preferred_element_type=jnp.float32)
                + rope_square
            )
            inverse = lax.rsqrt(sums * (1.0 / 96) + eps)
            part = part * low_gain * inverse
            if pair == 0:
                inverse = pltpu.roll(inverse, 64, 1)
                keys = [
                    jnp.where(lane < 64, part, rope_at[0] * inverse),
                    jnp.where(
                        (lane >= 32) & (lane < 64), rope_at[1] * inverse, pltpu.roll(part, 32, 1)
                    ),
                ]
                value_first = [pltpu.roll(value, 96, 1), value]
                value_second = [pltpu.roll(value, 64, 1), pltpu.roll(value, 96, 1)]
                free = [lane >= 96, (lane >= 64) & (lane < 96)]
            else:
                keys = [
                    jnp.where(lane < 64, rope_at[2] * inverse, pltpu.roll(part, 64, 1)),
                    jnp.where(lane >= 96, rope_at[3] * inverse, pltpu.roll(part, 96, 1)),
                ]
                value_first = [pltpu.roll(value, 32, 1), pltpu.roll(value, 64, 1)]
                value_second = [value, pltpu.roll(value, 32, 1)]
                free = [(lane >= 32) & (lane < 64), lane < 32]
            for odd in range(2):
                head = four * 4 + pair * 2 + odd
                span = slice(head * rows, (head + 1) * rows)
                head_query = query_at[pair * 2 + odd]
                out[span, 0:128] = jnp.where(free[odd], value_first[odd], head_query).astype(
                    jnp.bfloat16
                )
                out[span, 128:256] = jnp.where(free[odd], value_second[odd], keys[odd]).astype(
                    jnp.bfloat16
                )


def attend_kernel(start, packed, out):
    length = packed.shape[0]
    rows = 256
    scale = 96 ** (-0.5)
    begin = start[0]
    keep = (((lane_iota(16) - begin + 128) % 128) < 96).astype(jnp.float32).astype(jnp.bfloat16)[0:1]
    query_seg = lax.broadcasted_iota(jnp.int32, (rows, rows), 0) // SPAN
    key_seg = lax.broadcasted_iota(jnp.int32, (rows, rows), 1) // SPAN
    allowed = key_seg <= query_seg
    lane = lane_iota(64)
    to_front = (160 - begin) % 128

    def fold(array, combine):
        parts = [array[:, at : at + 128] for at in range(0, array.shape[1], 128)]
        while len(parts) > 1:
            parts = [combine(*parts[at : at + 2]) if at + 1 < len(parts) else parts[at] for at in range(0, len(parts), 2)]
        return parts[0]

    for block in range(length // rows):
        first, last = block * rows, (block + 1) * rows
        head_query = packed[first:last, 0:128] * keep
        scores = lax.dot_general(
            head_query,
            packed[0:last, 128:256],
            (((1,), (1,)), ((), ())),
            preferred_element_type=jnp.float32,
        )
        own = jnp.where(allowed, scores[:, first:last], -1e30)
        if block:
            scores = jnp.concatenate([scores[:, :first], own], axis=1)
        else:
            scores = own
        top = jnp.max(fold(scores, jnp.maximum), axis=-1, keepdims=True)
        raised = jnp.exp((scores - top) * scale)
        row_sum = jnp.sum(fold(raised, jnp.add), axis=-1, keepdims=True)
        summed = jnp.dot(
            raised.astype(jnp.bfloat16), packed[0:last, :], preferred_element_type=jnp.float32
        )
        summed = summed * (1.0 / row_sum)
        for half in range(2):
            low = summed[half * 128 : half * 128 + 64]
            high = summed[half * 128 + 64 : half * 128 + 128]
            joined = jnp.where(
                lane < 64,
                jnp.where(
                    lane < 32,
                    pltpu.roll(low[:, :128], to_front, 1),
                    pltpu.roll(low[:, 128:], (to_front + 32) % 128, 1),
                ),
                jnp.where(
                    lane < 96,
                    pltpu.roll(high[:, :128], (to_front + 64) % 128, 1),
                    pltpu.roll(high[:, 128:], (to_front + 96) % 128, 1),
                ),
            )
            at = (block * 2 + half) * 64
            out[at : at + 64, :] = joined.astype(jnp.bfloat16)


def route_kernel(choice, group_prob, shares, spread, gather, weight):
    tokens = choice.shape[1]
    expert = lax.broadcasted_iota(jnp.int32, (LANES, tokens), 0)
    first = choice[0:1, :]
    second = choice[1:2, :]
    hot_first = (expert == first).astype(jnp.float32)
    hot_second = (expert == second).astype(jnp.float32)
    earlier = (
        (lax.broadcasted_iota(jnp.int32, (tokens, tokens), 0) < lane_iota(tokens, tokens))
        .astype(jnp.float32)
        .astype(jnp.bfloat16)
    )
    count_first = jnp.dot(
        hot_first.astype(jnp.bfloat16), earlier, preferred_element_type=jnp.float32
    )
    count_second = jnp.dot(
        hot_second.astype(jnp.bfloat16), earlier, preferred_element_type=jnp.float32
    ) + jnp.sum(hot_first, axis=1, keepdims=True)
    rank_first = jnp.sum(count_first * hot_first, axis=0, keepdims=True).astype(jnp.int32)
    rank_second = jnp.sum(count_second * hot_second, axis=0, keepdims=True).astype(jnp.int32)
    row_first = first * 8 + rank_first
    row_second = second * 8 + rank_second
    slot_row = lax.broadcasted_iota(jnp.int32, (spread.shape[0], tokens), 0)
    for half in range(2):
        picked = (slot_row == row_first + 4 * half) | (slot_row == row_second + 4 * half)
        spread[:, half * 128 : half * 128 + 128] = picked.astype(jnp.float32).astype(jnp.bfloat16)
    wide = lane_iota(tokens, 512)

    def down(row):
        return jnp.broadcast_to(row.astype(jnp.float32), (tokens, tokens)).T[:, 0:1]

    for k, (chosen, rank) in enumerate(((first, rank_first), (second, rank_second))):
        target = down(chosen * SLOTS + rank).astype(jnp.int32)
        gather[k * tokens : (k + 1) * tokens, :] = (
            (target == wide).astype(jnp.float32).astype(jnp.bfloat16)
        )
    total = shares[0:1, :] + shares[1:2, :]
    weight[:, 0:1] = down(group_prob[...] * shares[0:1, :] / total)
    weight[:, 1:2] = down(group_prob[...] * shares[1:2, :] / total)


def mix_kernel(
    arrived, residual, mix_gain, out_weight, ffn_gain, spread, stream_out, outgoing, heads_out
):
    tokens = residual.shape[0]
    half_rows = tokens // 2
    lane = lane_iota(half_rows)
    width = residual.shape[1]
    square_low = jnp.zeros((half_rows, 1), jnp.float32)
    square_high = jnp.zeros((half_rows, 1), jnp.float32)
    pairs = arrived.shape[0] // tokens
    for pair in range(pairs):
        one = arrived[pair * tokens : pair * tokens + half_rows, :].astype(jnp.float32)
        two = arrived[pair * tokens + half_rows : (pair + 1) * tokens, :].astype(jnp.float32)
        low = jnp.where(lane < 64, one, pltpu.roll(two, 64, 1))
        high = jnp.where(lane < 64, pltpu.roll(one, 64, 1), two)
        square_low = square_low + jnp.sum(low * low, axis=-1, keepdims=True)
        square_high = square_high + jnp.sum(high * high, axis=-1, keepdims=True)
        heads_out[0:half_rows, pair * 128 : pair * 128 + 128] = low
        heads_out[half_rows:tokens, pair * 128 : pair * 128 + 128] = high
    squares = jnp.concatenate([square_low, square_high], axis=0)
    inverse = lax.rsqrt(squares * (1.0 / heads_out.shape[1]) + eps)
    mixed_in = (heads_out[...] * inverse * mix_gain[...]).astype(jnp.bfloat16)
    stream = residual[...].astype(jnp.float32) + jnp.dot(
        mixed_in, out_weight[...], preferred_element_type=jnp.float32
    )
    stream_out[...] = stream
    normed = (stream * inverse_rms(stream, width) * ffn_gain[...]).astype(jnp.bfloat16)
    stacked = jnp.concatenate([normed[:, : width // 2], normed[:, width // 2 :]], axis=0)
    outgoing[...] = jnp.dot(
        spread[...], stacked, preferred_element_type=jnp.float32
    ).astype(jnp.bfloat16)


def unstack(blocks, rows_out):
    pairs, width = blocks.shape[0] // 16, blocks.shape[1]
    view = blocks[...].astype(jnp.float32).reshape(pairs, 2, 8, width)
    one, two = view[:, 0], view[:, 1]
    upper = lax.broadcasted_iota(jnp.int32, (pairs, 8, width), 1) < 4
    low = jnp.where(upper, one, pltpu.roll(two, 4, 1))
    high = jnp.where(upper, pltpu.roll(one, 4, 1), two)
    rows_out[:, 0:width] = low.reshape(pairs * 8, width).astype(jnp.bfloat16)
    rows_out[:, width : 2 * width] = high.reshape(pairs * 8, width).astype(jnp.bfloat16)


def expert_kernel(arrived, gate_weight, up_weight, down_weight, out, rows_in):
    unstack(arrived, rows_in)
    gate_act = jnp.dot(rows_in[...], gate_weight[0], preferred_element_type=jnp.float32)
    upward = jnp.dot(rows_in[...], up_weight[0], preferred_element_type=jnp.float32)
    hidden = (jax.nn.silu(gate_act) * upward).astype(jnp.bfloat16)
    expert_out = jnp.dot(hidden, down_weight[0], preferred_element_type=jnp.float32)
    rows, width = expert_out.shape
    width = width // 2
    low = expert_out[:, :width].reshape(rows // 8, 8, width)
    high = expert_out[:, width:].reshape(rows // 8, 8, width)
    upper = lax.broadcasted_iota(jnp.int32, (rows // 8, 8, width), 1) < 4
    one = jnp.where(upper, low, pltpu.roll(high, 4, 1))
    two = jnp.where(upper, pltpu.roll(low, 4, 1), high)
    both = jnp.concatenate([one[:, None], two[:, None]], axis=1)
    out[...] = both.reshape(rows * 2, width).astype(jnp.bfloat16)


def combine_kernel(returned, gather, stream, route_weight, out, rows_back):
    unstack(returned, rows_back)
    tokens = stream.shape[0]
    picked = jnp.dot(gather[...], rows_back[...], preferred_element_type=jnp.float32)
    routed = route_weight[:, 0:1] * picked[:tokens] + route_weight[:, 1:2] * picked[tokens:]
    out[...] = (stream[...] + routed).astype(jnp.bfloat16)


def call(body, out_shapes, mib, scratch=(), name=None, scalars=0):
    spec = [pl.BlockSpec(memory_space=pltpu.SMEM)] * scalars
    extra = {}

    def run(*operands):
        if scalars:
            extra["in_specs"] = spec + [
                pl.BlockSpec(memory_space=pltpu.VMEM) for _ in operands[scalars:]
            ]
        return pl.pallas_call(
            body,
            out_shape=out_shapes,
            scratch_shapes=list(scratch),
            compiler_params=pltpu.CompilerParams(vmem_limit_bytes=mib * 2**20),
            name=name,
            **extra,
        )(*operands)

    return run


def per_device(
    residual,
    query,
    latent,
    rope_key,
    latent_gain,
    query_gain,
    key_gain,
    key_weight,
    value_weight,
    mix_gain,
    out_weight,
    ffn_gain,
    expert_choice,
    group_prob,
    expert_prob,
    gate_weight,
    up_weight,
    down_weight,
):
    tokens = residual.shape[1]
    width = residual.shape[2]
    sequence = tokens * lax.axis_size("sp")
    shape = jax.ShapeDtypeStruct
    phases = angles(lax.axis_index("sp") * tokens, tokens, rope_key.shape[2])
    packed = call(
        project_kernel,
        shape((16 * tokens, 256), jnp.bfloat16),
        12,
        scratch=(pltpu.VMEM((16, 128), jnp.float32), pltpu.VMEM((tokens, 384), jnp.float32)),
        name="project",
    )(
        query[0],
        latent[0],
        rope_key[0].T,
        latent_gain[None],
        query_gain[None],
        key_gain[None],
        jnp.cos(phases),
        jnp.sin(phases),
        key_weight,
        value_weight,
    )
    by_head = lax.all_to_all(packed, "sp", split_axis=0, concat_axis=0, tiled=True)
    spread, gather, route_weight = call(
        route_kernel,
        (
            shape((1024, 256), jnp.bfloat16),
            shape((256, 512), jnp.bfloat16),
            shape((tokens, 2), jnp.float32),
        ),
        8,
        name="route",
    )(expert_choice[0].T, group_prob, expert_prob[0].T)
    start = (lax.axis_index("sp") * 96) % 128
    head_out = call(
        attend_kernel, shape((sequence // 2, 128), jnp.bfloat16), 20, name="attend", scalars=1
    )(start[None].astype(jnp.int32), by_head)
    by_token = lax.all_to_all(head_out, "sp", split_axis=0, concat_axis=0, tiled=True)
    stream, outgoing = call(
        mix_kernel,
        (shape((tokens, width), jnp.float32), shape((1024, 1024), jnp.bfloat16)),
        16,
        scratch=(pltpu.VMEM((tokens, 1024), jnp.float32),),
        name="mix",
    )(by_token, residual[0], mix_gain[None], out_weight, ffn_gain[None], spread)
    arrived = lax.all_to_all(outgoing, ("sp", "dp"), split_axis=0, concat_axis=0, tiled=True)
    answers = call(
        expert_kernel,
        shape((1024, 1024), jnp.bfloat16),
        20,
        scratch=(pltpu.VMEM((512, width), jnp.bfloat16),),
        name="expert",
    )(arrived, gate_weight, up_weight, down_weight)
    returned = lax.all_to_all(answers, ("sp", "dp"), split_axis=0, concat_axis=0, tiled=True)
    return call(
        combine_kernel,
        shape((tokens, width), jnp.bfloat16),
        14,
        scratch=(pltpu.VMEM((512, width), jnp.bfloat16),),
        name="combine",
    )(returned, gather, stream, route_weight)[None]


def solution(mesh):
    return jax.shard_map(
        per_device,
        mesh=mesh,
        in_specs=(
            P("dp", "sp", None),
            P("dp", "sp", None),
            P("dp", "sp", None),
            P("dp", "sp", None),
            P(),
            P(),
            P(),
            P(),
            P(),
            P(),
            P(),
            P(),
            P("dp", "sp", None),
            P("dp", "sp"),
            P("dp", "sp", None),
            P(("sp", "dp"), None, None),
            P(("sp", "dp"), None, None),
            P(("sp", "dp"), None, None),
        ),
        out_specs=P("dp", "sp", None),
        check_vma=False,
    )
```

```python
import jax
import jax.numpy as jnp
from jax import lax
from jax.experimental import pallas as pl
from jax.experimental.pallas import tpu as pltpu
from jax.sharding import PartitionSpec as P

SPAN = 64
LANES = 128
SLOTS = 4

eps = 1e-06


def angles(offset, span_count, rope_width):
    position = (offset + jnp.arange(span_count, dtype=jnp.int32)).astype(jnp.float32)
    frequency = 10000.0 ** (-2.0 * jnp.arange(rope_width // 2, dtype=jnp.float32) / rope_width)
    return position[:, None] * frequency[None, :]


def lane_iota(rows, width=LANES):
    return lax.broadcasted_iota(jnp.int32, (rows, width), 1)


def inverse_rms(vector, width):
    return lax.rsqrt(jnp.sum(vector * vector, axis=-1, keepdims=True) * (1.0 / width) + eps)


def turn_lanes(vector, cos_part, minus_sin, plus_sin):
    return (
        vector * cos_part
        + pltpu.roll(vector, 112, 1) * minus_sin
        + pltpu.roll(vector, 16, 1) * plus_sin
    )


def split_high_low(vector):
    high = vector.astype(jnp.bfloat16)
    low = (vector - high.astype(jnp.float32)).astype(jnp.bfloat16)
    return jnp.concatenate([high, low], axis=1)


def same_group(group_of_row, group_of_lane):
    ones = (group_of_row == group_of_lane).astype(jnp.float32).astype(jnp.bfloat16)
    return jnp.concatenate([ones, ones], axis=0)


def project_kernel(
    query,
    latent,
    rope,
    latent_gain,
    query_gain,
    key_gain,
    cos_table,
    sin_table,
    key_weight,
    value_weight,
    out,
    query_here,
    latent_here,
    rope_here,
    latent_gain_here,
    query_gain_here,
    key_gain_here,
    key_weight_here,
    value_weight_here,
    arrivals,
    small,
    turn,
):
    moves = [
        pltpu.make_async_copy(source, target, arrivals.at[k])
        for k, (source, target) in enumerate(
            (
                (query_gain, query_gain_here),
                (key_gain, key_gain_here),
                (rope, rope_here),
                (latent_gain, latent_gain_here),
                (latent, latent_here),
                (key_weight, key_weight_here),
                (value_weight, value_weight_here),
                (query, query_here),
            )
        )
    ]
    for move in moves:
        move.start()
    for move in moves:
        move.wait()
    query, latent, rope, latent_gain = query_here, latent_here, rope_here, latent_gain_here
    query_gain, key_gain = query_gain_here, key_gain_here
    key_weight, value_weight = key_weight_here, value_weight_here
    rows = query.shape[0]
    heads = query.shape[1] // 96
    lane = lane_iota(rows)
    raw_latent = latent[...].astype(jnp.float32)
    normed_latent = (
        raw_latent * inverse_rms(raw_latent, raw_latent.shape[1]) * latent_gain[...]
    ).astype(jnp.bfloat16)
    key_part = (
        jnp.dot(normed_latent, key_weight[...], preferred_element_type=jnp.float32)
        .astype(jnp.bfloat16)
        .astype(jnp.float32)
    )
    values = jnp.dot(normed_latent, value_weight[...], preferred_element_type=jnp.float32)

    small[...] = jnp.zeros(small.shape, jnp.float32)
    small[0:1, 0:96] = query_gain[...]
    small[8:9, 0:96] = key_gain[...]
    turn[:, 0:128] = jnp.ones((rows, 128), jnp.float32)
    turn[:, 128:384] = jnp.zeros((rows, 256), jnp.float32)
    turn[:, 64:80] = cos_table[...]
    turn[:, 80:96] = cos_table[...]
    turn[:, 192:208] = -sin_table[...]
    turn[:, 336:352] = sin_table[...]
    tables = [turn[:, 0:128], turn[:, 128:256], turn[:, 256:384]]
    gain_row = small[0:8, :]
    key_gain_row = small[8:9, :]
    gain_tiles = [
        (gain_row + pltpu.roll(gain_row, 96, 1) * (lane_iota(8) >= 96).astype(jnp.float32))[0:1],
        jnp.where(lane_iota(8) < 64, pltpu.roll(gain_row, 96, 1), pltpu.roll(gain_row, 64, 1))[0:1],
        jnp.where(lane_iota(8) < 32, pltpu.roll(gain_row, 64, 1), pltpu.roll(gain_row, 32, 1))[0:1],
    ]
    turn_tiles = [
        tables,
        [pltpu.roll(t, 96, 1) for t in tables],
        [jnp.where(lane < 64, pltpu.roll(t, 64, 1), pltpu.roll(t, 32, 1)) for t in tables],
    ]
    wide_row = lax.broadcasted_iota(jnp.int32, (128, 256), 0)
    wide_lane = lax.broadcasted_iota(jnp.int32, (128, 256), 1)
    sum_low = same_group(wide_row // 96, wide_lane // 96)
    sum_mid = same_group((wide_row + 128) // 96, wide_lane // 96)
    sum_mid_last = same_group(
        (lax.broadcasted_iota(jnp.int32, (128, 128), 0) + 128) // 96, (lane_iota(128) + 256) // 96
    )
    sum_high = same_group((wide_row + 256) // 96, (wide_lane + 128) // 96)
    sum_pair = same_group(
        lax.broadcasted_iota(jnp.int32, (128, 128), 0) // 64, lane_iota(128) // 64
    )
    sum_all = jnp.ones((256, 128), jnp.bfloat16)

    place = (
        lax.broadcasted_iota(jnp.int32, (32, LANES), 0) + 64 == lane_iota(32)
    ).astype(jnp.float32).astype(jnp.bfloat16)
    rope_part = lax.dot_general(
        rope[...], place, (((0,), (0,)), ((), ())), preferred_element_type=jnp.float32
    )
    rope_square = jnp.dot(
        split_high_low(rope_part * rope_part), sum_all, preferred_element_type=jnp.float32
    )
    rope_turned = turn_lanes(rope_part * key_gain_row, *tables)
    rope_at = [rope_turned] + [pltpu.roll(rope_turned, shift, 1) for shift in (96, 64, 32)]
    low_gain = jnp.where(lane_iota(8) < 64, small[8:16, :], pltpu.roll(small[8:16, :], 64, 1))[0:1]

    for four in range(heads // 4):
        raw = [
            query[:, four * 384 + t * 128 : four * 384 + t * 128 + 128].astype(jnp.float32)
            for t in range(3)
        ]
        squares = [split_high_low(t * t) for t in raw]
        from_low = jnp.dot(squares[0], sum_low, preferred_element_type=jnp.float32)
        from_mid = jnp.dot(squares[1], sum_mid, preferred_element_type=jnp.float32)
        from_mid_last = jnp.dot(squares[1], sum_mid_last, preferred_element_type=jnp.float32)
        from_high = jnp.dot(squares[2], sum_high, preferred_element_type=jnp.float32)
        sums = [
            from_low[:, :128] + from_mid[:, :128],
            from_low[:, 128:] + from_mid[:, 128:] + from_high[:, :128],
            from_mid_last + from_high[:, 128:],
        ]
        turned = [
            turn_lanes(
                raw[t] * lax.rsqrt(sums[t] * (1.0 / 96) + eps) * gain_tiles[t], *turn_tiles[t]
            )
            for t in range(3)
        ]
        query_at = [
            turned[0],
            jnp.where(lane < 96, turned[1], turned[0]),
            jnp.where(lane < 64, turned[2], turned[1]),
            turned[2],
        ]
        for pair in range(2):
            at = (four * 2 + pair) * 128
            part = key_part[:, at : at + 128]
            value = values[:, at : at + 128]
            sums = (
                jnp.dot(split_high_low(part * part), sum_pair, preferred_element_type=jnp.float32)
                + rope_square
            )
            inverse = lax.rsqrt(sums * (1.0 / 96) + eps)
            part = part * low_gain * inverse
            if pair == 0:
                inverse = pltpu.roll(inverse, 64, 1)
                keys = [
                    jnp.where(lane < 64, part, rope_at[0] * inverse),
                    jnp.where(
                        (lane >= 32) & (lane < 64), rope_at[1] * inverse, pltpu.roll(part, 32, 1)
                    ),
                ]
                value_first = [pltpu.roll(value, 96, 1), value]
                value_second = [pltpu.roll(value, 64, 1), pltpu.roll(value, 96, 1)]
                free = [lane >= 96, (lane >= 64) & (lane < 96)]
            else:
                keys = [
                    jnp.where(lane < 64, rope_at[2] * inverse, pltpu.roll(part, 64, 1)),
                    jnp.where(lane >= 96, rope_at[3] * inverse, pltpu.roll(part, 96, 1)),
                ]
                value_first = [pltpu.roll(value, 32, 1), pltpu.roll(value, 64, 1)]
                value_second = [value, pltpu.roll(value, 32, 1)]
                free = [(lane >= 32) & (lane < 64), lane < 32]
            for odd in range(2):
                head = four * 4 + pair * 2 + odd
                span = slice(head * rows, (head + 1) * rows)
                head_query = query_at[pair * 2 + odd]
                out[span, 0:128] = jnp.where(free[odd], value_first[odd], head_query).astype(
                    jnp.bfloat16
                )
                out[span, 128:256] = jnp.where(free[odd], value_second[odd], keys[odd]).astype(
                    jnp.bfloat16
                )


def attend_kernel(
    packed,
    choice,
    group_prob,
    shares,
    out_weight,
    gate_weight,
    up_weight,
    down_weight,
    out,
    spread,
    gather,
    weight,
    out_weight_here,
    gate_weight_here,
    up_weight_here,
    down_weight_here,
    arrivals,
):
    moves = [
        pltpu.make_async_copy(source, target, arrivals.at[k])
        for k, (source, target) in enumerate(
            (
                (out_weight, out_weight_here),
                (gate_weight, gate_weight_here),
                (up_weight, up_weight_here),
                (down_weight, down_weight_here),
            )
        )
    ]
    for move in moves:
        move.start()
    route(choice, group_prob, shares, spread, gather, weight)
    attend(packed, out)
    for move in moves:
        move.wait()


def attend(packed, out):
    length = packed.shape[0]
    rows = 256
    scale = 96 ** (-0.5) * 1.4426950408889634
    begin = (lax.axis_index("sp") * 96) % 128
    keep = (((lane_iota(16) - begin + 128) % 128) < 96).astype(jnp.float32).astype(jnp.bfloat16)[0:1]
    query_seg = lax.broadcasted_iota(jnp.int32, (rows, rows), 0) // SPAN
    key_seg = lax.broadcasted_iota(jnp.int32, (rows, rows), 1) // SPAN
    allowed = key_seg <= query_seg
    lane = lane_iota(64)
    to_front = (160 - begin) % 128

    def fold(array, combine):
        parts = [array[:, at : at + 128] for at in range(0, array.shape[1], 128)]
        while len(parts) > 1:
            parts = [combine(*parts[at : at + 2]) if at + 1 < len(parts) else parts[at] for at in range(0, len(parts), 2)]
        return parts[0]

    for block in range(length // rows):
        first, last = block * rows, (block + 1) * rows
        head_query = packed[first:last, 0:128] * keep
        scores = lax.dot_general(
            head_query,
            packed[0:last, 128:256],
            (((1,), (1,)), ((), ())),
            preferred_element_type=jnp.float32,
        )
        own = jnp.where(allowed, scores[:, first:last], -1e30)
        if block:
            scores = jnp.concatenate([scores[:, :first], own], axis=1)
        else:
            scores = own
        top = jnp.max(fold(scores, jnp.maximum), axis=-1, keepdims=True)
        raised = jnp.exp2(scores * scale - top * scale)
        row_sum = jnp.sum(fold(raised, jnp.add), axis=-1, keepdims=True)
        summed = jnp.dot(
            raised.astype(jnp.bfloat16), packed[0:last, :], preferred_element_type=jnp.float32
        )
        summed = summed * (1.0 / row_sum)
        for half in range(2):
            low = summed[half * 128 : half * 128 + 64]
            high = summed[half * 128 + 64 : half * 128 + 128]
            joined = jnp.where(
                lane < 64,
                jnp.where(
                    lane < 32,
                    pltpu.roll(low[:, :128], to_front, 1),
                    pltpu.roll(low[:, 128:], (to_front + 32) % 128, 1),
                ),
                jnp.where(
                    lane < 96,
                    pltpu.roll(high[:, :128], (to_front + 64) % 128, 1),
                    pltpu.roll(high[:, 128:], (to_front + 96) % 128, 1),
                ),
            )
            at = (block * 2 + half) * 64
            out[at : at + 64, :] = joined.astype(jnp.bfloat16)


def route(choice, group_prob, shares, spread, gather, weight):
    tokens = choice.shape[1]
    expert = lax.broadcasted_iota(jnp.int32, (LANES, tokens), 0)
    first = choice[0:1, :]
    second = choice[1:2, :]
    hot_first = (expert == first).astype(jnp.float32)
    hot_second = (expert == second).astype(jnp.float32)
    earlier = (
        (lax.broadcasted_iota(jnp.int32, (tokens, tokens), 0) < lane_iota(tokens, tokens))
        .astype(jnp.float32)
        .astype(jnp.bfloat16)
    )
    count_first = jnp.dot(
        hot_first.astype(jnp.bfloat16), earlier, preferred_element_type=jnp.float32
    )
    count_second = jnp.dot(
        hot_second.astype(jnp.bfloat16), earlier, preferred_element_type=jnp.float32
    ) + jnp.sum(hot_first, axis=1, keepdims=True)
    rank_first = jnp.sum(count_first * hot_first, axis=0, keepdims=True).astype(jnp.int32)
    rank_second = jnp.sum(count_second * hot_second, axis=0, keepdims=True).astype(jnp.int32)
    row_first = first * 8 + rank_first
    row_second = second * 8 + rank_second
    slot_row = lax.broadcasted_iota(jnp.int32, (spread.shape[0], tokens), 0)
    for half in range(2):
        picked = (slot_row == row_first + 4 * half) | (slot_row == row_second + 4 * half)
        spread[:, half * 128 : half * 128 + 128] = picked.astype(jnp.float32).astype(jnp.bfloat16)
    wide = lane_iota(tokens, 512)

    def down(row):
        return jnp.broadcast_to(row.astype(jnp.float32), (tokens, tokens)).T[:, 0:1]

    for k, (chosen, rank) in enumerate(((first, rank_first), (second, rank_second))):
        target = down(chosen * SLOTS + rank).astype(jnp.int32)
        gather[k * tokens : (k + 1) * tokens, :] = (
            (target == wide).astype(jnp.float32).astype(jnp.bfloat16)
        )
    total = shares[0:1, :] + shares[1:2, :]
    weight[:, 0:1] = down(group_prob[...] * shares[0:1, :] / total)
    weight[:, 1:2] = down(group_prob[...] * shares[1:2, :] / total)


def mix_kernel(
    arrived, residual, mix_gain, out_weight, ffn_gain, spread, stream_out, outgoing, heads_out
):
    tokens = residual.shape[0]
    half_rows = tokens // 2
    lane = lane_iota(half_rows)
    width = residual.shape[1]
    square_low = jnp.zeros((half_rows, 1), jnp.float32)
    square_high = jnp.zeros((half_rows, 1), jnp.float32)
    pairs = arrived.shape[0] // tokens
    for pair in range(pairs):
        one = arrived[pair * tokens : pair * tokens + half_rows, :].astype(jnp.float32)
        two = arrived[pair * tokens + half_rows : (pair + 1) * tokens, :].astype(jnp.float32)
        low = jnp.where(lane < 64, one, pltpu.roll(two, 64, 1))
        high = jnp.where(lane < 64, pltpu.roll(one, 64, 1), two)
        square_low = square_low + jnp.sum(low * low, axis=-1, keepdims=True)
        square_high = square_high + jnp.sum(high * high, axis=-1, keepdims=True)
        heads_out[0:half_rows, pair * 128 : pair * 128 + 128] = low
        heads_out[half_rows:tokens, pair * 128 : pair * 128 + 128] = high
    squares = jnp.concatenate([square_low, square_high], axis=0)
    inverse = lax.rsqrt(squares * (1.0 / heads_out.shape[1]) + eps)
    mixed_in = (heads_out[...] * inverse * mix_gain[...]).astype(jnp.bfloat16)
    stream = residual[...].astype(jnp.float32) + jnp.dot(
        mixed_in, out_weight[...], preferred_element_type=jnp.float32
    )
    stream_out[...] = stream
    normed = (stream * inverse_rms(stream, width) * ffn_gain[...]).astype(jnp.bfloat16)
    stacked = jnp.concatenate([normed[:, : width // 2], normed[:, width // 2 :]], axis=0)
    outgoing[...] = jnp.dot(
        spread[...], stacked, preferred_element_type=jnp.float32
    ).astype(jnp.bfloat16)


def unstack(blocks, rows_out):
    pairs, width = blocks.shape[0] // 16, blocks.shape[1]
    view = blocks[...].astype(jnp.float32).reshape(pairs, 2, 8, width)
    one, two = view[:, 0], view[:, 1]
    upper = lax.broadcasted_iota(jnp.int32, (pairs, 8, width), 1) < 4
    low = jnp.where(upper, one, pltpu.roll(two, 4, 1))
    high = jnp.where(upper, pltpu.roll(one, 4, 1), two)
    rows_out[:, 0:width] = low.reshape(pairs * 8, width).astype(jnp.bfloat16)
    rows_out[:, width : 2 * width] = high.reshape(pairs * 8, width).astype(jnp.bfloat16)


def expert_kernel(arrived, gate_weight, up_weight, down_weight, out, rows_in):
    unstack(arrived, rows_in)
    gate_act = jnp.dot(rows_in[...], gate_weight[0], preferred_element_type=jnp.float32)
    upward = jnp.dot(rows_in[...], up_weight[0], preferred_element_type=jnp.float32)
    hidden = (jax.nn.silu(gate_act) * upward).astype(jnp.bfloat16)
    expert_out = jnp.dot(hidden, down_weight[0], preferred_element_type=jnp.float32)
    rows, width = expert_out.shape
    width = width // 2
    low = expert_out[:, :width].reshape(rows // 8, 8, width)
    high = expert_out[:, width:].reshape(rows // 8, 8, width)
    upper = lax.broadcasted_iota(jnp.int32, (rows // 8, 8, width), 1) < 4
    one = jnp.where(upper, low, pltpu.roll(high, 4, 1))
    two = jnp.where(upper, pltpu.roll(low, 4, 1), high)
    both = jnp.concatenate([one[:, None], two[:, None]], axis=1)
    out[...] = both.reshape(rows * 2, width).astype(jnp.bfloat16)


def combine_kernel(returned, gather, stream, route_weight, out, rows_back):
    unstack(returned, rows_back)
    tokens = stream.shape[0]
    picked = jnp.dot(gather[...], rows_back[...], preferred_element_type=jnp.float32)
    routed = route_weight[:, 0:1] * picked[:tokens] + route_weight[:, 1:2] * picked[tokens:]
    out[...] = (stream[...] + routed).astype(jnp.bfloat16)


VMEM = pl.BlockSpec(memory_space=pltpu.VMEM)
HBM = pl.BlockSpec(memory_space=pltpu.HBM)


def call(body, in_specs, out_shapes, mib, scratch=(), name=None):
    many = isinstance(out_shapes, tuple)
    run = pl.pallas_call(
        body,
        in_specs=in_specs,
        out_shape=out_shapes,
        out_specs=tuple(VMEM for _ in out_shapes) if many else VMEM,
        scratch_shapes=list(scratch),
        compiler_params=pltpu.CompilerParams(vmem_limit_bytes=mib * 2**20),
        name=name,
    )

    def placed(*operands):
        return run(
            *(
                pltpu.with_memory_space_constraint(x, pltpu.HBM) if spec is HBM else x
                for spec, x in zip(in_specs, operands)
            )
        )

    return placed


def per_device(
    residual,
    query,
    latent,
    rope_key,
    latent_gain,
    query_gain,
    key_gain,
    key_weight,
    value_weight,
    mix_gain,
    out_weight,
    ffn_gain,
    expert_choice,
    group_prob,
    expert_prob,
    gate_weight,
    up_weight,
    down_weight,
):
    tokens = residual.shape[1]
    width = residual.shape[2]
    sequence = tokens * lax.axis_size("sp")
    shape = jax.ShapeDtypeStruct
    phases = angles(lax.axis_index("sp") * tokens, tokens, rope_key.shape[2])
    half = jnp.bfloat16
    packed = call(
        project_kernel,
        [HBM] * 6 + [VMEM] * 2 + [HBM] * 2,
        shape((16 * tokens, 256), half),
        14,
        scratch=(
            pltpu.VMEM(query.shape[1:], half),
            pltpu.VMEM(latent.shape[1:], half),
            pltpu.VMEM(rope_key.shape[:0:-1], half),
            pltpu.VMEM((1,) + latent_gain.shape, jnp.float32),
            pltpu.VMEM((1,) + query_gain.shape, jnp.float32),
            pltpu.VMEM((1,) + key_gain.shape, jnp.float32),
            pltpu.VMEM(key_weight.shape, half),
            pltpu.VMEM(value_weight.shape, half),
            pltpu.SemaphoreType.DMA((8,)),
            pltpu.VMEM((16, 128), jnp.float32),
            pltpu.VMEM((tokens, 384), jnp.float32),
        ),
        name="project",
    )(
        query[0],
        latent[0],
        rope_key[0].T,
        latent_gain[None],
        query_gain[None],
        key_gain[None],
        jnp.cos(phases),
        jnp.sin(phases),
        key_weight,
        value_weight,
    )
    by_head = lax.all_to_all(packed, "sp", split_axis=0, concat_axis=0, tiled=True)
    head_out, spread, gather, route_weight, out_weight, gate_weight, up_weight, down_weight = call(
        attend_kernel,
        [VMEM] * 4 + [HBM] * 4,
        (
            shape((sequence // 2, 128), half),
            shape((1024, 256), half),
            shape((256, 512), half),
            shape((tokens, 2), jnp.float32),
            shape(out_weight.shape, half),
            shape(gate_weight.shape, half),
            shape(up_weight.shape, half),
            shape(down_weight.shape, half),
        ),
        30,
        scratch=(pltpu.SemaphoreType.DMA((4,)),),
        name="attend",
    )(
        by_head,
        expert_choice[0].T,
        group_prob,
        expert_prob[0].T,
        out_weight,
        gate_weight,
        up_weight,
        down_weight,
    )
    by_token = lax.all_to_all(head_out, "sp", split_axis=0, concat_axis=0, tiled=True)
    stream, outgoing = call(
        mix_kernel,
        [VMEM] * 6,
        (shape((tokens, width), jnp.float32), shape((1024, 1024), half)),
        16,
        scratch=(pltpu.VMEM((tokens, 1024), jnp.float32),),
        name="mix",
    )(by_token, residual[0], mix_gain[None], out_weight, ffn_gain[None], spread)
    arrived = lax.all_to_all(outgoing, ("sp", "dp"), split_axis=0, concat_axis=0, tiled=True)
    answers = call(
        expert_kernel,
        [VMEM] * 4,
        shape((1024, 1024), half),
        20,
        scratch=(pltpu.VMEM((512, width), half),),
        name="expert",
    )(arrived, gate_weight, up_weight, down_weight)
    returned = lax.all_to_all(answers, ("sp", "dp"), split_axis=0, concat_axis=0, tiled=True)
    return call(
        combine_kernel,
        [VMEM] * 4,
        shape((tokens, width), half),
        14,
        scratch=(pltpu.VMEM((512, width), half),),
        name="combine",
    )(returned, gather, stream, route_weight)[None]


def solution(mesh):
    return jax.shard_map(
        per_device,
        mesh=mesh,
        in_specs=(
            P("dp", "sp", None),
            P("dp", "sp", None),
            P("dp", "sp", None),
            P("dp", "sp", None),
            P(),
            P(),
            P(),
            P(),
            P(),
            P(),
            P(),
            P(),
            P("dp", "sp", None),
            P("dp", "sp"),
            P("dp", "sp", None),
            P(("sp", "dp"), None, None),
            P(("sp", "dp"), None, None),
            P(("sp", "dp"), None, None),
        ),
        out_specs=P("dp", "sp", None),
        check_vma=False,
    )
```

```python
import jax
import jax.numpy as jnp
from jax import lax
from jax.experimental import pallas as pl
from jax.experimental.pallas import tpu as pltpu
from jax.sharding import PartitionSpec as P

SPAN = 64
LANES = 128
SLOTS = 4

eps = 1e-06


def angles(offset, span_count, rope_width):
    position = (offset + jnp.arange(span_count, dtype=jnp.int32)).astype(jnp.float32)
    frequency = 10000.0 ** (-2.0 * jnp.arange(rope_width // 2, dtype=jnp.float32) / rope_width)
    return position[:, None] * frequency[None, :]


def lane_iota(rows, width=LANES):
    return lax.broadcasted_iota(jnp.int32, (rows, width), 1)


def inverse_rms(vector, width):
    return lax.rsqrt(jnp.sum(vector * vector, axis=-1, keepdims=True) * (1.0 / width) + eps)


def turn_lanes(vector, cos_part, minus_sin, plus_sin):
    return (
        vector * cos_part
        + pltpu.roll(vector, 112, 1) * minus_sin
        + pltpu.roll(vector, 16, 1) * plus_sin
    )


def split_high_low(vector):
    high = vector.astype(jnp.bfloat16)
    low = (vector - high.astype(jnp.float32)).astype(jnp.bfloat16)
    return jnp.concatenate([high, low], axis=1)


def same_group(group_of_row, group_of_lane):
    ones = (group_of_row == group_of_lane).astype(jnp.float32).astype(jnp.bfloat16)
    return jnp.concatenate([ones, ones], axis=0)


def project_kernel(
    query,
    latent,
    rope,
    latent_gain,
    query_gain,
    key_gain,
    cos_table,
    sin_table,
    key_weight,
    value_weight,
    out,
    query_here,
    latent_here,
    rope_here,
    latent_gain_here,
    query_gain_here,
    key_gain_here,
    key_weight_here,
    value_weight_here,
    arrivals,
    small,
    turn,
):
    moves = [
        pltpu.make_async_copy(source, target, arrivals.at[k])
        for k, (source, target) in enumerate(
            (
                (query_gain, query_gain_here),
                (key_gain, key_gain_here),
                (rope, rope_here),
                (latent_gain, latent_gain_here),
                (latent, latent_here),
                (key_weight, key_weight_here),
                (value_weight, value_weight_here),
                (query, query_here),
            )
        )
    ]
    for move in moves:
        move.start()
    for move in moves[:3]:
        move.wait()
    query, latent, rope, latent_gain = query_here, latent_here, rope_here, latent_gain_here
    query_gain, key_gain = query_gain_here, key_gain_here
    key_weight, value_weight = key_weight_here, value_weight_here
    rows = query.shape[0]
    heads = query.shape[1] // 96
    lane = lane_iota(rows)
    small[...] = jnp.zeros(small.shape, jnp.float32)
    small[0:1, 0:96] = query_gain[...]
    small[8:9, 0:96] = key_gain[...]
    turn[:, 0:128] = jnp.ones((rows, 128), jnp.float32)
    turn[:, 128:384] = jnp.zeros((rows, 256), jnp.float32)
    turn[:, 64:80] = cos_table[...]
    turn[:, 80:96] = cos_table[...]
    turn[:, 192:208] = -sin_table[...]
    turn[:, 336:352] = sin_table[...]
    tables = [turn[:, 0:128], turn[:, 128:256], turn[:, 256:384]]
    gain_row = small[0:8, :]
    key_gain_row = small[8:9, :]
    gain_tiles = [
        (gain_row + pltpu.roll(gain_row, 96, 1) * (lane_iota(8) >= 96).astype(jnp.float32))[0:1],
        jnp.where(lane_iota(8) < 64, pltpu.roll(gain_row, 96, 1), pltpu.roll(gain_row, 64, 1))[0:1],
        jnp.where(lane_iota(8) < 32, pltpu.roll(gain_row, 64, 1), pltpu.roll(gain_row, 32, 1))[0:1],
    ]
    turn_tiles = [
        tables,
        [pltpu.roll(t, 96, 1) for t in tables],
        [jnp.where(lane < 64, pltpu.roll(t, 64, 1), pltpu.roll(t, 32, 1)) for t in tables],
    ]
    wide_row = lax.broadcasted_iota(jnp.int32, (128, 256), 0)
    wide_lane = lax.broadcasted_iota(jnp.int32, (128, 256), 1)
    sum_low = same_group(wide_row // 96, wide_lane // 96)
    sum_mid = same_group((wide_row + 128) // 96, wide_lane // 96)
    sum_mid_last = same_group(
        (lax.broadcasted_iota(jnp.int32, (128, 128), 0) + 128) // 96, (lane_iota(128) + 256) // 96
    )
    sum_high = same_group((wide_row + 256) // 96, (wide_lane + 128) // 96)
    sum_pair = same_group(
        lax.broadcasted_iota(jnp.int32, (128, 128), 0) // 64, lane_iota(128) // 64
    )
    sum_all = jnp.ones((256, 128), jnp.bfloat16)

    place = (
        lax.broadcasted_iota(jnp.int32, (32, LANES), 0) + 64 == lane_iota(32)
    ).astype(jnp.float32).astype(jnp.bfloat16)
    rope_part = lax.dot_general(
        rope[...], place, (((0,), (0,)), ((), ())), preferred_element_type=jnp.float32
    )
    rope_square = jnp.dot(
        split_high_low(rope_part * rope_part), sum_all, preferred_element_type=jnp.float32
    )
    rope_turned = turn_lanes(rope_part * key_gain_row, *tables)
    rope_at = [rope_turned] + [pltpu.roll(rope_turned, shift, 1) for shift in (96, 64, 32)]
    low_gain = jnp.where(lane_iota(8) < 64, small[8:16, :], pltpu.roll(small[8:16, :], 64, 1))[0:1]

    for move in moves[3:7]:
        move.wait()
    raw_latent = latent[...].astype(jnp.float32)
    normed_latent = (
        raw_latent * inverse_rms(raw_latent, raw_latent.shape[1]) * latent_gain[...]
    ).astype(jnp.bfloat16)
    key_part = (
        jnp.dot(normed_latent, key_weight[...], preferred_element_type=jnp.float32)
        .astype(jnp.bfloat16)
        .astype(jnp.float32)
    )
    values = jnp.dot(normed_latent, value_weight[...], preferred_element_type=jnp.float32)
    moves[7].wait()

    for four in range(heads // 4):
        raw = [
            query[:, four * 384 + t * 128 : four * 384 + t * 128 + 128].astype(jnp.float32)
            for t in range(3)
        ]
        squares = [split_high_low(t * t) for t in raw]
        from_low = jnp.dot(squares[0], sum_low, preferred_element_type=jnp.float32)
        from_mid = jnp.dot(squares[1], sum_mid, preferred_element_type=jnp.float32)
        from_mid_last = jnp.dot(squares[1], sum_mid_last, preferred_element_type=jnp.float32)
        from_high = jnp.dot(squares[2], sum_high, preferred_element_type=jnp.float32)
        sums = [
            from_low[:, :128] + from_mid[:, :128],
            from_low[:, 128:] + from_mid[:, 128:] + from_high[:, :128],
            from_mid_last + from_high[:, 128:],
        ]
        turned = [
            turn_lanes(
                raw[t] * lax.rsqrt(sums[t] * (1.0 / 96) + eps) * gain_tiles[t], *turn_tiles[t]
            )
            for t in range(3)
        ]
        query_at = [
            turned[0],
            jnp.where(lane < 96, turned[1], turned[0]),
            jnp.where(lane < 64, turned[2], turned[1]),
            turned[2],
        ]
        for pair in range(2):
            at = (four * 2 + pair) * 128
            part = key_part[:, at : at + 128]
            value = values[:, at : at + 128]
            sums = (
                jnp.dot(split_high_low(part * part), sum_pair, preferred_element_type=jnp.float32)
                + rope_square
            )
            inverse = lax.rsqrt(sums * (1.0 / 96) + eps)
            part = part * low_gain * inverse
            if pair == 0:
                inverse = pltpu.roll(inverse, 64, 1)
                keys = [
                    jnp.where(lane < 64, part, rope_at[0] * inverse),
                    jnp.where(
                        (lane >= 32) & (lane < 64), rope_at[1] * inverse, pltpu.roll(part, 32, 1)
                    ),
                ]
                value_first = [pltpu.roll(value, 96, 1), value]
                value_second = [pltpu.roll(value, 64, 1), pltpu.roll(value, 96, 1)]
                free = [lane >= 96, (lane >= 64) & (lane < 96)]
            else:
                keys = [
                    jnp.where(lane < 64, rope_at[2] * inverse, pltpu.roll(part, 64, 1)),
                    jnp.where(lane >= 96, rope_at[3] * inverse, pltpu.roll(part, 96, 1)),
                ]
                value_first = [pltpu.roll(value, 32, 1), pltpu.roll(value, 64, 1)]
                value_second = [value, pltpu.roll(value, 32, 1)]
                free = [(lane >= 32) & (lane < 64), lane < 32]
            for odd in range(2):
                head = four * 4 + pair * 2 + odd
                span = slice(head * rows, (head + 1) * rows)
                head_query = query_at[pair * 2 + odd]
                out[span, 0:128] = jnp.where(free[odd], value_first[odd], head_query).astype(
                    jnp.bfloat16
                )
                out[span, 128:256] = jnp.where(free[odd], value_second[odd], keys[odd]).astype(
                    jnp.bfloat16
                )


def attend_kernel(
    packed,
    choice,
    group_prob,
    shares,
    out_weight,
    out,
    spread,
    gather,
    weight,
    out_weight_here,
    arrival,
):
    move = pltpu.make_async_copy(out_weight, out_weight_here, arrival)
    move.start()
    route(choice, group_prob, shares, spread, gather, weight)
    attend(packed, out)
    move.wait()


def attend(packed, out):
    length = packed.shape[0]
    rows = 256
    scale = 96 ** (-0.5) * 1.4426950408889634
    begin = (lax.axis_index("sp") * 96) % 128
    keep = (((lane_iota(16) - begin + 128) % 128) < 96).astype(jnp.float32).astype(jnp.bfloat16)[0:1]
    query_seg = lax.broadcasted_iota(jnp.int32, (rows, rows), 0) // SPAN
    key_seg = lax.broadcasted_iota(jnp.int32, (rows, rows), 1) // SPAN
    allowed = key_seg <= query_seg
    lane = lane_iota(64)
    to_front = (160 - begin) % 128

    def fold(array, combine):
        parts = [array[:, at : at + 128] for at in range(0, array.shape[1], 128)]
        while len(parts) > 1:
            parts = [combine(*parts[at : at + 2]) if at + 1 < len(parts) else parts[at] for at in range(0, len(parts), 2)]
        return parts[0]

    def scores_of(block):
        first, last = block * rows, (block + 1) * rows
        return lax.dot_general(
            packed[first:last, 0:128] * keep,
            packed[0:last, 128:256],
            (((1,), (1,)), ((), ())),
            preferred_element_type=jnp.float32,
        )

    blocks = length // rows
    coming = scores_of(blocks - 1)
    for block in range(blocks - 1, -1, -1):
        first, last = block * rows, (block + 1) * rows
        scores = coming
        if block:
            coming = scores_of(block - 1)
        own = jnp.where(allowed, scores[:, first:last], -1e30)
        scores = jnp.concatenate([scores[:, :first], own], axis=1) if block else own
        top = jnp.max(fold(scores, jnp.maximum), axis=-1, keepdims=True)
        raised = jnp.exp2(scores * scale - top * scale)
        row_sum = jnp.sum(fold(raised, jnp.add), axis=-1, keepdims=True)
        summed = jnp.dot(
            raised.astype(jnp.bfloat16), packed[0:last, :], preferred_element_type=jnp.float32
        )
        summed = summed * (1.0 / row_sum)
        for half in range(2):
            low = summed[half * 128 : half * 128 + 64]
            high = summed[half * 128 + 64 : half * 128 + 128]
            joined = jnp.where(
                lane < 64,
                jnp.where(
                    lane < 32,
                    pltpu.roll(low[:, :128], to_front, 1),
                    pltpu.roll(low[:, 128:], (to_front + 32) % 128, 1),
                ),
                jnp.where(
                    lane < 96,
                    pltpu.roll(high[:, :128], (to_front + 64) % 128, 1),
                    pltpu.roll(high[:, 128:], (to_front + 96) % 128, 1),
                ),
            )
            at = (block * 2 + half) * 64
            out[at : at + 64, :] = joined.astype(jnp.bfloat16)


def route(choice, group_prob, shares, spread, gather, weight):
    tokens = choice.shape[1]
    expert = lax.broadcasted_iota(jnp.int32, (LANES, tokens), 0)
    first = choice[0:1, :]
    second = choice[1:2, :]
    hot_first = (expert == first).astype(jnp.float32)
    hot_second = (expert == second).astype(jnp.float32)
    earlier = (
        (lax.broadcasted_iota(jnp.int32, (tokens, tokens), 0) < lane_iota(tokens, tokens))
        .astype(jnp.float32)
        .astype(jnp.bfloat16)
    )
    count_first = jnp.dot(
        hot_first.astype(jnp.bfloat16), earlier, preferred_element_type=jnp.float32
    )
    count_second = jnp.dot(
        hot_second.astype(jnp.bfloat16), earlier, preferred_element_type=jnp.float32
    ) + jnp.sum(hot_first, axis=1, keepdims=True)
    rank_first = jnp.sum(count_first * hot_first, axis=0, keepdims=True).astype(jnp.int32)
    rank_second = jnp.sum(count_second * hot_second, axis=0, keepdims=True).astype(jnp.int32)
    row_first = first * 8 + rank_first
    row_second = second * 8 + rank_second
    slot_row = lax.broadcasted_iota(jnp.int32, (spread.shape[0], tokens), 0)
    for half in range(2):
        picked = (slot_row == row_first + 4 * half) | (slot_row == row_second + 4 * half)
        spread[:, half * 128 : half * 128 + 128] = picked.astype(jnp.float32).astype(jnp.bfloat16)
    wide = lane_iota(tokens, 512)

    def down(row):
        return jnp.broadcast_to(row.astype(jnp.float32), (tokens, tokens)).T[:, 0:1]

    for k, (chosen, rank) in enumerate(((first, rank_first), (second, rank_second))):
        target = down(chosen * SLOTS + rank).astype(jnp.int32)
        gather[k * tokens : (k + 1) * tokens, :] = (
            (target == wide).astype(jnp.float32).astype(jnp.bfloat16)
        )
    total = shares[0:1, :] + shares[1:2, :]
    weight[:, 0:1] = down(group_prob[...] * shares[0:1, :] / total)
    weight[:, 1:2] = down(group_prob[...] * shares[1:2, :] / total)


def mix_kernel(
    arrived, residual, mix_gain, out_weight, ffn_gain, spread, stream_out, outgoing, heads_out
):
    tokens = residual.shape[0]
    half_rows = tokens // 2
    lane = lane_iota(half_rows)
    width = residual.shape[1]
    square_low = jnp.zeros((half_rows, 1), jnp.float32)
    square_high = jnp.zeros((half_rows, 1), jnp.float32)
    pairs = arrived.shape[0] // tokens
    for pair in range(pairs):
        one = arrived[pair * tokens : pair * tokens + half_rows, :].astype(jnp.float32)
        two = arrived[pair * tokens + half_rows : (pair + 1) * tokens, :].astype(jnp.float32)
        low = jnp.where(lane < 64, one, pltpu.roll(two, 64, 1))
        high = jnp.where(lane < 64, pltpu.roll(one, 64, 1), two)
        square_low = square_low + jnp.sum(low * low, axis=-1, keepdims=True)
        square_high = square_high + jnp.sum(high * high, axis=-1, keepdims=True)
        heads_out[0:half_rows, pair * 128 : pair * 128 + 128] = low
        heads_out[half_rows:tokens, pair * 128 : pair * 128 + 128] = high
    squares = jnp.concatenate([square_low, square_high], axis=0)
    inverse = lax.rsqrt(squares * (1.0 / heads_out.shape[1]) + eps)
    mixed_in = (heads_out[...] * inverse * mix_gain[...]).astype(jnp.bfloat16)
    stream = residual[...].astype(jnp.float32) + jnp.dot(
        mixed_in, out_weight[...], preferred_element_type=jnp.float32
    )
    stream_out[...] = stream
    normed = (stream * inverse_rms(stream, width) * ffn_gain[...]).astype(jnp.bfloat16)
    stacked = jnp.concatenate([normed[:, : width // 2], normed[:, width // 2 :]], axis=0)
    outgoing[...] = jnp.dot(
        spread[...], stacked, preferred_element_type=jnp.float32
    ).astype(jnp.bfloat16)


def unstack(blocks, rows_out):
    pairs, width = blocks.shape[0] // 16, blocks.shape[1]
    view = blocks[...].astype(jnp.float32).reshape(pairs, 2, 8, width)
    one, two = view[:, 0], view[:, 1]
    upper = lax.broadcasted_iota(jnp.int32, (pairs, 8, width), 1) < 4
    low = jnp.where(upper, one, pltpu.roll(two, 4, 1))
    high = jnp.where(upper, pltpu.roll(one, 4, 1), two)
    rows_out[:, 0:width] = low.reshape(pairs * 8, width).astype(jnp.bfloat16)
    rows_out[:, width : 2 * width] = high.reshape(pairs * 8, width).astype(jnp.bfloat16)


def expert_kernel(arrived, gate_weight, up_weight, down_weight, out, rows_in):
    unstack(arrived, rows_in)
    gate_act = jnp.dot(rows_in[...], gate_weight[0], preferred_element_type=jnp.float32)
    upward = jnp.dot(rows_in[...], up_weight[0], preferred_element_type=jnp.float32)
    hidden = (jax.nn.silu(gate_act) * upward).astype(jnp.bfloat16)
    expert_out = jnp.dot(hidden, down_weight[0], preferred_element_type=jnp.float32)
    rows, width = expert_out.shape
    width = width // 2
    low = expert_out[:, :width].reshape(rows // 8, 8, width)
    high = expert_out[:, width:].reshape(rows // 8, 8, width)
    upper = lax.broadcasted_iota(jnp.int32, (rows // 8, 8, width), 1) < 4
    one = jnp.where(upper, low, pltpu.roll(high, 4, 1))
    two = jnp.where(upper, pltpu.roll(low, 4, 1), high)
    both = jnp.concatenate([one[:, None], two[:, None]], axis=1)
    out[...] = both.reshape(rows * 2, width).astype(jnp.bfloat16)


def combine_kernel(returned, gather, stream, route_weight, out, rows_back):
    unstack(returned, rows_back)
    tokens = stream.shape[0]
    picked = jnp.dot(gather[...], rows_back[...], preferred_element_type=jnp.float32)
    routed = route_weight[:, 0:1] * picked[:tokens] + route_weight[:, 1:2] * picked[tokens:]
    out[...] = (stream[...] + routed).astype(jnp.bfloat16)


VMEM = pl.BlockSpec(memory_space=pltpu.VMEM)
HBM = pl.BlockSpec(memory_space=pltpu.HBM)


def call(body, in_specs, out_shapes, mib, scratch=(), name=None):
    many = isinstance(out_shapes, tuple)
    run = pl.pallas_call(
        body,
        in_specs=in_specs,
        out_shape=out_shapes,
        out_specs=tuple(VMEM for _ in out_shapes) if many else VMEM,
        scratch_shapes=list(scratch),
        compiler_params=pltpu.CompilerParams(vmem_limit_bytes=mib * 2**20),
        name=name,
    )

    def placed(*operands):
        return run(
            *(
                pltpu.with_memory_space_constraint(x, pltpu.HBM) if spec is HBM else x
                for spec, x in zip(in_specs, operands)
            )
        )

    return placed


def per_device(
    residual,
    query,
    latent,
    rope_key,
    latent_gain,
    query_gain,
    key_gain,
    key_weight,
    value_weight,
    mix_gain,
    out_weight,
    ffn_gain,
    expert_choice,
    group_prob,
    expert_prob,
    gate_weight,
    up_weight,
    down_weight,
):
    tokens = residual.shape[1]
    width = residual.shape[2]
    sequence = tokens * lax.axis_size("sp")
    shape = jax.ShapeDtypeStruct
    phases = angles(lax.axis_index("sp") * tokens, tokens, rope_key.shape[2])
    half = jnp.bfloat16
    packed = call(
        project_kernel,
        [HBM] * 6 + [VMEM] * 2 + [HBM] * 2,
        shape((16 * tokens, 256), half),
        14,
        scratch=(
            pltpu.VMEM(query.shape[1:], half),
            pltpu.VMEM(latent.shape[1:], half),
            pltpu.VMEM(rope_key.shape[:0:-1], half),
            pltpu.VMEM((1,) + latent_gain.shape, jnp.float32),
            pltpu.VMEM((1,) + query_gain.shape, jnp.float32),
            pltpu.VMEM((1,) + key_gain.shape, jnp.float32),
            pltpu.VMEM(key_weight.shape, half),
            pltpu.VMEM(value_weight.shape, half),
            pltpu.SemaphoreType.DMA((8,)),
            pltpu.VMEM((16, 128), jnp.float32),
            pltpu.VMEM((tokens, 384), jnp.float32),
        ),
        name="project",
    )(
        query[0],
        latent[0],
        rope_key[0].T,
        latent_gain[None],
        query_gain[None],
        key_gain[None],
        jnp.cos(phases),
        jnp.sin(phases),
        key_weight,
        value_weight,
    )
    by_head = lax.all_to_all(packed, "sp", split_axis=0, concat_axis=0, tiled=True)
    head_out, spread, gather, route_weight, out_weight = call(
        attend_kernel,
        [VMEM] * 4 + [HBM],
        (
            shape((sequence // 2, 128), half),
            shape((1024, 256), half),
            shape((256, 512), half),
            shape((tokens, 2), jnp.float32),
            shape(out_weight.shape, half),
        ),
        24,
        scratch=(pltpu.SemaphoreType.DMA,),
        name="attend",
    )(by_head, expert_choice[0].T, group_prob, expert_prob[0].T, out_weight)
    by_token = lax.all_to_all(head_out, "sp", split_axis=0, concat_axis=0, tiled=True)
    stream, outgoing = call(
        mix_kernel,
        [VMEM] * 6,
        (shape((tokens, width), jnp.float32), shape((1024, 1024), half)),
        16,
        scratch=(pltpu.VMEM((tokens, 1024), jnp.float32),),
        name="mix",
    )(by_token, residual[0], mix_gain[None], out_weight, ffn_gain[None], spread)
    arrived = lax.all_to_all(outgoing, ("sp", "dp"), split_axis=0, concat_axis=0, tiled=True)
    answers = call(
        expert_kernel,
        [VMEM] * 4,
        shape((1024, 1024), half),
        20,
        scratch=(pltpu.VMEM((512, width), half),),
        name="expert",
    )(arrived, gate_weight, up_weight, down_weight)
    returned = lax.all_to_all(answers, ("sp", "dp"), split_axis=0, concat_axis=0, tiled=True)
    return call(
        combine_kernel,
        [VMEM] * 4,
        shape((tokens, width), half),
        14,
        scratch=(pltpu.VMEM((512, width), half),),
        name="combine",
    )(returned, gather, stream, route_weight)[None]


def solution(mesh):
    return jax.shard_map(
        per_device,
        mesh=mesh,
        in_specs=(
            P("dp", "sp", None),
            P("dp", "sp", None),
            P("dp", "sp", None),
            P("dp", "sp", None),
            P(),
            P(),
            P(),
            P(),
            P(),
            P(),
            P(),
            P(),
            P("dp", "sp", None),
            P("dp", "sp"),
            P("dp", "sp", None),
            P(("sp", "dp"), None, None),
            P(("sp", "dp"), None, None),
            P(("sp", "dp"), None, None),
        ),
        out_specs=P("dp", "sp", None),
        check_vma=False,
    )
```

```python
import jax
import jax.numpy as jnp
from jax import lax
from jax.experimental import pallas as pl
from jax.experimental.pallas import tpu as pltpu
from jax.sharding import PartitionSpec as P

SPAN = 64
LANES = 128
SLOTS = 4

eps = 1e-06


def angles(offset, span_count, rope_width):
    position = (offset + jnp.arange(span_count, dtype=jnp.int32)).astype(jnp.float32)
    frequency = 10000.0 ** (-2.0 * jnp.arange(rope_width // 2, dtype=jnp.float32) / rope_width)
    return position[:, None] * frequency[None, :]


def lane_iota(rows, width=LANES):
    return lax.broadcasted_iota(jnp.int32, (rows, width), 1)


def inverse_rms(vector, width):
    return lax.rsqrt(jnp.sum(vector * vector, axis=-1, keepdims=True) * (1.0 / width) + eps)


def turn_lanes(vector, cos_part, minus_sin, plus_sin):
    return (
        vector * cos_part
        + pltpu.roll(vector, 112, 1) * minus_sin
        + pltpu.roll(vector, 16, 1) * plus_sin
    )


def split_high_low(vector):
    high = vector.astype(jnp.bfloat16)
    low = (vector - high.astype(jnp.float32)).astype(jnp.bfloat16)
    return jnp.concatenate([high, low], axis=1)


def same_group(group_of_row, group_of_lane):
    ones = (group_of_row == group_of_lane).astype(jnp.float32).astype(jnp.bfloat16)
    return jnp.concatenate([ones, ones], axis=0)


def route(choice, group_prob, shares, spread, gather, weight):
    tokens = choice.shape[1]
    expert = lax.broadcasted_iota(jnp.int32, (LANES, tokens), 0)
    first = choice[0:1, :]
    second = choice[1:2, :]
    hot_first = (expert == first).astype(jnp.float32)
    hot_second = (expert == second).astype(jnp.float32)
    earlier = (
        (lax.broadcasted_iota(jnp.int32, (tokens, tokens), 0) < lane_iota(tokens, tokens))
        .astype(jnp.float32)
        .astype(jnp.bfloat16)
    )
    count_first = jnp.dot(
        hot_first.astype(jnp.bfloat16), earlier, preferred_element_type=jnp.float32
    )
    count_second = jnp.dot(
        hot_second.astype(jnp.bfloat16), earlier, preferred_element_type=jnp.float32
    ) + jnp.sum(hot_first, axis=1, keepdims=True)
    rank_first = jnp.sum(count_first * hot_first, axis=0, keepdims=True).astype(jnp.int32)
    rank_second = jnp.sum(count_second * hot_second, axis=0, keepdims=True).astype(jnp.int32)
    row_first = first * 8 + rank_first
    row_second = second * 8 + rank_second
    slot_row = lax.broadcasted_iota(jnp.int32, (spread.shape[0], tokens), 0)
    for half in range(2):
        picked = (slot_row == row_first + 4 * half) | (slot_row == row_second + 4 * half)
        spread[:, half * 128 : half * 128 + 128] = picked.astype(jnp.float32).astype(jnp.bfloat16)
    wide = lane_iota(tokens, 512)

    def down(row):
        return jnp.broadcast_to(row.astype(jnp.float32), (tokens, tokens)).T[:, 0:1]

    for k, (chosen, rank) in enumerate(((first, rank_first), (second, rank_second))):
        target = down(chosen * SLOTS + rank).astype(jnp.int32)
        gather[k * tokens : (k + 1) * tokens, :] = (
            (target == wide).astype(jnp.float32).astype(jnp.bfloat16)
        )
    total = shares[0:1, :] + shares[1:2, :]
    weight[:, 0:1] = down(group_prob[...] * shares[0:1, :] / total)
    weight[:, 1:2] = down(group_prob[...] * shares[1:2, :] / total)


def start_moves(pairs, arrivals):
    moves = [
        pltpu.make_async_copy(source, target, arrivals.at[k])
        for k, (source, target) in enumerate(pairs)
    ]
    for move in moves:
        move.start()
    return moves


def pack_kernel(latent, rope, latent_gain, out, latent_here, rope_here, latent_gain_here, arrivals):
    moves = start_moves(
        ((latent_gain, latent_gain_here), (rope, rope_here), (latent, latent_here)), arrivals
    )
    for move in moves:
        move.wait()
    rows = latent_here.shape[0]
    raw = latent_here[...].astype(jnp.float32)
    normed = (raw * inverse_rms(raw, raw.shape[1]) * latent_gain_here[...]).astype(jnp.bfloat16)
    block = rows + 16
    first, second = rope_here[0:16, :], rope_here[16:32, :]
    for device in range(out.shape[0] // block):
        at = device * block
        out[at : at + rows, :] = normed
        out[at + rows : at + block, 0:128] = first
        out[at + rows : at + block, 128:256] = second


def query_kernel(
    query,
    query_gain,
    key_weight,
    cos_table,
    sin_table,
    choice,
    group_prob,
    shares,
    out,
    key_weight_turned,
    spread,
    gather,
    weight,
    query_here,
    query_gain_here,
    key_weight_here,
    arrivals,
    small,
    turn,
):
    moves = start_moves(
        (
            (query_gain, query_gain_here),
            (query, query_here),
            (key_weight, key_weight_here),
        ),
        arrivals,
    )
    route(choice, group_prob, shares, spread, gather, weight)
    query = query_here
    rows = query.shape[0]
    heads = query.shape[1] // 96
    lane = lane_iota(rows)
    early = lax.broadcasted_iota(jnp.int32, (rows, LANES), 0) < SPAN
    for move in moves:
        move.wait()
    key_weight_turned[...] = key_weight_here[...].astype(jnp.float32).T.astype(jnp.bfloat16)
    small[...] = jnp.zeros(small.shape, jnp.float32)
    small[0:1, 0:96] = query_gain_here[...]
    turn[:, 0:128] = jnp.ones((rows, 128), jnp.float32)
    turn[:, 128:384] = jnp.zeros((rows, 256), jnp.float32)
    turn[:, 64:80] = cos_table[...]
    turn[:, 80:96] = cos_table[...]
    turn[:, 192:208] = -sin_table[...]
    turn[:, 336:352] = sin_table[...]
    tables = [turn[:, 0:128], turn[:, 128:256], turn[:, 256:384]]
    gain_row = small[0:8, :]
    gain_tiles = [
        (gain_row + pltpu.roll(gain_row, 96, 1) * (lane_iota(8) >= 96).astype(jnp.float32))[0:1],
        jnp.where(lane_iota(8) < 64, pltpu.roll(gain_row, 96, 1), pltpu.roll(gain_row, 64, 1))[0:1],
        jnp.where(lane_iota(8) < 32, pltpu.roll(gain_row, 64, 1), pltpu.roll(gain_row, 32, 1))[0:1],
    ]
    turn_tiles = [
        tables,
        [pltpu.roll(t, 96, 1) for t in tables],
        [jnp.where(lane < 64, pltpu.roll(t, 64, 1), pltpu.roll(t, 32, 1)) for t in tables],
    ]
    wide_row = lax.broadcasted_iota(jnp.int32, (128, 256), 0)
    wide_lane = lax.broadcasted_iota(jnp.int32, (128, 256), 1)
    sum_low = same_group(wide_row // 96, wide_lane // 96)
    sum_mid = same_group((wide_row + 128) // 96, wide_lane // 96)
    sum_mid_last = same_group(
        (lax.broadcasted_iota(jnp.int32, (128, 128), 0) + 128) // 96, (lane_iota(128) + 256) // 96
    )
    sum_high = same_group((wide_row + 256) // 96, (wide_lane + 128) // 96)

    def masking(begin):
        return jnp.where(
            lane == begin, 1.0, jnp.where((lane == begin + 1) & early, 1.0, 0.0)
        )

    free = [lane >= 96, (lane >= 64) & (lane < 96), (lane >= 32) & (lane < 64), lane < 32]
    selects = [masking(begin) for begin in (96, 64, 32, 0)]
    for four in range(heads // 4):
        raw = [
            query[:, four * 384 + t * 128 : four * 384 + t * 128 + 128].astype(jnp.float32)
            for t in range(3)
        ]
        squares = [split_high_low(t * t) for t in raw]
        from_low = jnp.dot(squares[0], sum_low, preferred_element_type=jnp.float32)
        from_mid = jnp.dot(squares[1], sum_mid, preferred_element_type=jnp.float32)
        from_mid_last = jnp.dot(squares[1], sum_mid_last, preferred_element_type=jnp.float32)
        from_high = jnp.dot(squares[2], sum_high, preferred_element_type=jnp.float32)
        sums = [
            from_low[:, :128] + from_mid[:, :128],
            from_low[:, 128:] + from_mid[:, 128:] + from_high[:, :128],
            from_mid_last + from_high[:, 128:],
        ]
        turned = [
            turn_lanes(
                raw[t] * lax.rsqrt(sums[t] * (1.0 / 96) + eps) * gain_tiles[t], *turn_tiles[t]
            )
            for t in range(3)
        ]
        query_at = [
            turned[0],
            jnp.where(lane < 96, turned[1], turned[0]),
            jnp.where(lane < 64, turned[2], turned[1]),
            turned[2],
        ]
        for k in range(4):
            head = four * 4 + k
            out[head * rows : (head + 1) * rows, :] = jnp.where(
                free[k], selects[k], query_at[k]
            ).astype(jnp.bfloat16)


def attend_kernel(
    gathered,
    query,
    key_weight_turned,
    key_gain,
    cos_all,
    sin_all,
    value_weight_far,
    out_weight,
    out,
    out_weight_here,
    value_weight,
    latents,
    key_parts,
    keys,
    ropes,
    sums,
    arrivals,
):
    moves = start_moves(
        ((value_weight_far, value_weight), (out_weight, out_weight_here)), arrivals
    )
    own = lax.axis_index("sp")
    tokens = query.shape[0] // 16
    block = tokens + 16
    length = latents.shape[0]
    heads = key_weight_turned.shape[0] // 64
    scale = 96 ** (-0.5) * 1.4426950408889634
    half_gain = [key_gain[64:80, 0:1], key_gain[80:96, 0:1]]
    for device in range(length // tokens):
        at, here = device * block, slice(device * tokens, (device + 1) * tokens)
        latents[here, :] = gathered[at : at + tokens, :]
        first = gathered[at + tokens : at + block, 0:128].astype(jnp.float32)
        second = gathered[at + tokens : at + block, 128:256].astype(jnp.float32)
        sums[:, here] = jnp.sum(first * first + second * second, axis=0, keepdims=True)
        first, second = first * half_gain[0], second * half_gain[1]
        cos_part, sin_part = cos_all[:, here], sin_all[:, here]
        ropes[0:16, here] = first * cos_part - second * sin_part
        ropes[16:32, here] = second * cos_part + first * sin_part
    row = lax.broadcasted_iota(jnp.int32, (32, length), 0)
    key = lax.broadcasted_iota(jnp.int32, (32, length), 1)
    later = (row == 0) & (key >= (own + 1) * tokens)
    beside = (row == 1) & (key >= own * tokens + SPAN) & (key < (own + 1) * tokens)
    hidden = jnp.where(later | beside, -1e30, 0.0).astype(jnp.bfloat16)
    for k in range(4):
        keys[k, (96 * k + 96) % 128 : (96 * k + 96) % 128 + 32, :] = hidden
    for at in range(0, length, 256):
        key_parts[:, at : at + 256] = lax.dot_general(
            key_weight_turned[...],
            latents[at : at + 256, :],
            (((1,), (1,)), ((), ())),
            preferred_element_type=jnp.float32,
        ).astype(jnp.bfloat16)
    low_gain = jnp.broadcast_to(key_gain[0:64, 0:1], (64, 128))
    low_gain = jnp.concatenate([low_gain] * (length // 128), axis=1)

    def scores_of(head):
        part = key_parts[head * 64 : (head + 1) * 64, :].astype(jnp.float32)
        total = jnp.sum(part * part, axis=0, keepdims=True) + sums[...]
        inverse = lax.rsqrt(total * (1.0 / 96) + eps)
        part = (part * inverse * low_gain).astype(jnp.bfloat16)
        turned = (ropes[...] * inverse).astype(jnp.bfloat16)
        kind, begin = head % 4, (96 * head) % 128
        for piece, source in ((0, part[0:32]), (32, part[32:64]), (64, turned)):
            at = (begin + piece) % 128
            keys[kind, at : at + 32, :] = source
        return jnp.dot(
            query[head * tokens : (head + 1) * tokens, :],
            keys[kind],
            preferred_element_type=jnp.float32,
        )

    def fold(array, combine):
        parts = [array[:, at : at + 128] for at in range(0, array.shape[1], 128)]
        while len(parts) > 1:
            parts = [combine(*parts[at : at + 2]) for at in range(0, len(parts), 2)]
        return parts[0]

    lane = lane_iota(tokens)
    coming = scores_of(0)
    moves[0].wait()
    for head in range(heads):
        scores = coming
        if head + 1 < heads:
            coming = scores_of(head + 1)
        top = jnp.max(fold(scores, jnp.maximum), axis=-1, keepdims=True)
        raised = jnp.exp2(scores * scale - top * scale)
        row_sum = jnp.sum(fold(raised, jnp.add), axis=-1, keepdims=True)
        mixed = jnp.dot(
            raised.astype(jnp.bfloat16), latents[...], preferred_element_type=jnp.float32
        )
        mixed = (mixed * (1.0 / row_sum)).astype(jnp.bfloat16)
        pair = (head // 2) * 128
        both = jnp.dot(
            mixed, value_weight[:, pair : pair + 128], preferred_element_type=jnp.float32
        )
        if head % 2:
            out[:, pair : pair + 128] = jnp.where(lane < 64, before, both).astype(jnp.bfloat16)
        else:
            before = both
    moves[1].wait()


def mix_kernel(heads_out, residual, mix_gain, out_weight, ffn_gain, spread, stream_out, outgoing):
    width = residual.shape[1]
    wide = heads_out[...].astype(jnp.float32)
    mixed_in = (wide * inverse_rms(wide, wide.shape[1]) * mix_gain[...]).astype(jnp.bfloat16)
    stream = residual[...].astype(jnp.float32) + jnp.dot(
        mixed_in, out_weight[...], preferred_element_type=jnp.float32
    )
    stream_out[...] = stream
    normed = (stream * inverse_rms(stream, width) * ffn_gain[...]).astype(jnp.bfloat16)
    stacked = jnp.concatenate([normed[:, : width // 2], normed[:, width // 2 :]], axis=0)
    outgoing[...] = jnp.dot(
        spread[...], stacked, preferred_element_type=jnp.float32
    ).astype(jnp.bfloat16)


def unstack(blocks, rows_out):
    pairs, width = blocks.shape[0] // 16, blocks.shape[1]
    view = blocks[...].astype(jnp.float32).reshape(pairs, 2, 8, width)
    one, two = view[:, 0], view[:, 1]
    upper = lax.broadcasted_iota(jnp.int32, (pairs, 8, width), 1) < 4
    low = jnp.where(upper, one, pltpu.roll(two, 4, 1))
    high = jnp.where(upper, pltpu.roll(one, 4, 1), two)
    rows_out[:, 0:width] = low.reshape(pairs * 8, width).astype(jnp.bfloat16)
    rows_out[:, width : 2 * width] = high.reshape(pairs * 8, width).astype(jnp.bfloat16)


def expert_kernel(arrived, gate_weight, up_weight, down_weight, out, rows_in):
    unstack(arrived, rows_in)
    gate_act = jnp.dot(rows_in[...], gate_weight[0], preferred_element_type=jnp.float32)
    upward = jnp.dot(rows_in[...], up_weight[0], preferred_element_type=jnp.float32)
    hidden = (jax.nn.silu(gate_act) * upward).astype(jnp.bfloat16)
    expert_out = jnp.dot(hidden, down_weight[0], preferred_element_type=jnp.float32)
    rows, width = expert_out.shape
    width = width // 2
    low = expert_out[:, :width].reshape(rows // 8, 8, width)
    high = expert_out[:, width:].reshape(rows // 8, 8, width)
    upper = lax.broadcasted_iota(jnp.int32, (rows // 8, 8, width), 1) < 4
    one = jnp.where(upper, low, pltpu.roll(high, 4, 1))
    two = jnp.where(upper, pltpu.roll(low, 4, 1), high)
    both = jnp.concatenate([one[:, None], two[:, None]], axis=1)
    out[...] = both.reshape(rows * 2, width).astype(jnp.bfloat16)


def combine_kernel(returned, gather, stream, route_weight, out, rows_back):
    unstack(returned, rows_back)
    tokens = stream.shape[0]
    picked = jnp.dot(gather[...], rows_back[...], preferred_element_type=jnp.float32)
    routed = route_weight[:, 0:1] * picked[:tokens] + route_weight[:, 1:2] * picked[tokens:]
    out[...] = (stream[...] + routed).astype(jnp.bfloat16)


VMEM = pl.BlockSpec(memory_space=pltpu.VMEM)
HBM = pl.BlockSpec(memory_space=pltpu.HBM)


def call(body, in_specs, out_shapes, mib, scratch=(), name=None):
    many = isinstance(out_shapes, tuple)
    run = pl.pallas_call(
        body,
        in_specs=in_specs,
        out_shape=out_shapes,
        out_specs=tuple(VMEM for _ in out_shapes) if many else VMEM,
        scratch_shapes=list(scratch),
        compiler_params=pltpu.CompilerParams(vmem_limit_bytes=mib * 2**20),
        name=name,
    )

    def placed(*operands):
        return run(
            *(
                pltpu.with_memory_space_constraint(x, pltpu.HBM) if spec is HBM else x
                for spec, x in zip(in_specs, operands)
            )
        )

    return placed


def per_device(
    residual,
    query,
    latent,
    rope_key,
    latent_gain,
    query_gain,
    key_gain,
    key_weight,
    value_weight,
    mix_gain,
    out_weight,
    ffn_gain,
    expert_choice,
    group_prob,
    expert_prob,
    gate_weight,
    up_weight,
    down_weight,
):
    tokens = residual.shape[1]
    width = residual.shape[2]
    devices = lax.axis_size("sp")
    sequence = tokens * devices
    shape = jax.ShapeDtypeStruct
    half, full = jnp.bfloat16, jnp.float32
    block = tokens + 16
    packed = call(
        pack_kernel,
        [HBM] * 3,
        shape((devices * block, 256), half),
        6,
        scratch=(
            pltpu.VMEM(latent.shape[1:], half),
            pltpu.VMEM(rope_key.shape[:0:-1], half),
            pltpu.VMEM((1,) + latent_gain.shape, full),
            pltpu.SemaphoreType.DMA((3,)),
        ),
        name="pack",
    )(latent[0], rope_key[0].T, latent_gain[None])
    gathered = lax.all_to_all(packed, "sp", split_axis=0, concat_axis=0, tiled=True)
    own = angles(lax.axis_index("sp") * tokens, tokens, rope_key.shape[2])
    every = angles(0, sequence, rope_key.shape[2]).T
    (
        queries,
        key_weight_turned,
        spread,
        gather,
        route_weight,
    ) = call(
        query_kernel,
        [HBM] * 3 + [VMEM] * 5,
        (
            shape((16 * tokens, 128), half),
            shape(key_weight.shape[::-1], half),
            shape((1024, 256), half),
            shape((256, 512), half),
            shape((tokens, 2), full),
        ),
        22,
        scratch=(
            pltpu.VMEM(query.shape[1:], half),
            pltpu.VMEM((1,) + query_gain.shape, full),
            pltpu.VMEM(key_weight.shape, half),
            pltpu.SemaphoreType.DMA((3,)),
            pltpu.VMEM((8, 128), full),
            pltpu.VMEM((tokens, 384), full),
        ),
        name="query",
    )(
        query[0],
        query_gain[None],
        key_weight,
        jnp.cos(own),
        jnp.sin(own),
        expert_choice[0].T,
        group_prob,
        expert_prob[0].T,
    )
    heads_out, out_weight = call(
        attend_kernel,
        [VMEM] * 6 + [HBM] * 2,
        (shape((tokens, 1024), half), shape(out_weight.shape, half)),
        30,
        scratch=(
            pltpu.VMEM(value_weight.shape, half),
            pltpu.VMEM((sequence, 256), half),
            pltpu.VMEM((1024, sequence), half),
            pltpu.VMEM((4, 128, sequence), half),
            pltpu.VMEM((32, sequence), full),
            pltpu.VMEM((1, sequence), full),
            pltpu.SemaphoreType.DMA((2,)),
        ),
        name="attend",
    )(
        gathered,
        queries,
        key_weight_turned,
        key_gain[:, None],
        jnp.cos(every),
        jnp.sin(every),
        value_weight,
        out_weight,
    )
    stream, outgoing = call(
        mix_kernel,
        [VMEM] * 6,
        (shape((tokens, width), full), shape((1024, 1024), half)),
        16,
        name="mix",
    )(heads_out, residual[0], mix_gain[None], out_weight, ffn_gain[None], spread)
    arrived = lax.all_to_all(outgoing, ("sp", "dp"), split_axis=0, concat_axis=0, tiled=True)
    answers = call(
        expert_kernel,
        [VMEM] * 4,
        shape((1024, 1024), half),
        20,
        scratch=(pltpu.VMEM((512, width), half),),
        name="expert",
    )(arrived, gate_weight, up_weight, down_weight)
    returned = lax.all_to_all(answers, ("sp", "dp"), split_axis=0, concat_axis=0, tiled=True)
    return call(
        combine_kernel,
        [VMEM] * 4,
        shape((tokens, width), half),
        14,
        scratch=(pltpu.VMEM((512, width), half),),
        name="combine",
    )(returned, gather, stream, route_weight)[None]


def solution(mesh):
    return jax.shard_map(
        per_device,
        mesh=mesh,
        in_specs=(
            P("dp", "sp", None),
            P("dp", "sp", None),
            P("dp", "sp", None),
            P("dp", "sp", None),
            P(),
            P(),
            P(),
            P(),
            P(),
            P(),
            P(),
            P(),
            P("dp", "sp", None),
            P("dp", "sp"),
            P("dp", "sp", None),
            P(("sp", "dp"), None, None),
            P(("sp", "dp"), None, None),
            P(("sp", "dp"), None, None),
        ),
        out_specs=P("dp", "sp", None),
        check_vma=False,
    )
```

```python
import jax
import jax.numpy as jnp
from jax import lax
from jax.experimental import pallas as pl
from jax.experimental.pallas import tpu as pltpu
from jax.sharding import PartitionSpec as P

SPAN = 64
LANES = 128
SLOTS = 4

eps = 1e-06


def angles(offset, span_count, rope_width):
    position = (offset + jnp.arange(span_count, dtype=jnp.int32)).astype(jnp.float32)
    frequency = 10000.0 ** (-2.0 * jnp.arange(rope_width // 2, dtype=jnp.float32) / rope_width)
    return position[:, None] * frequency[None, :]


def lane_iota(rows, width=LANES):
    return lax.broadcasted_iota(jnp.int32, (rows, width), 1)


def inverse_rms(vector, width):
    return lax.rsqrt(jnp.sum(vector * vector, axis=-1, keepdims=True) * (1.0 / width) + eps)


def turn_lanes(vector, cos_part, minus_sin, plus_sin):
    return (
        vector * cos_part
        + pltpu.roll(vector, 112, 1) * minus_sin
        + pltpu.roll(vector, 16, 1) * plus_sin
    )


def split_high_low(vector):
    high = vector.astype(jnp.bfloat16)
    low = (vector - high.astype(jnp.float32)).astype(jnp.bfloat16)
    return jnp.concatenate([high, low], axis=1)


def same_group(group_of_row, group_of_lane):
    ones = (group_of_row == group_of_lane).astype(jnp.float32).astype(jnp.bfloat16)
    return jnp.concatenate([ones, ones], axis=0)


def route(choice, group_prob, shares, spread, gather, weight):
    tokens = choice.shape[1]
    expert = lax.broadcasted_iota(jnp.int32, (LANES, tokens), 0)
    first = choice[0:1, :]
    second = choice[1:2, :]
    hot_first = (expert == first).astype(jnp.float32)
    hot_second = (expert == second).astype(jnp.float32)
    earlier = (
        (lax.broadcasted_iota(jnp.int32, (tokens, tokens), 0) < lane_iota(tokens, tokens))
        .astype(jnp.float32)
        .astype(jnp.bfloat16)
    )
    count_first = jnp.dot(
        hot_first.astype(jnp.bfloat16), earlier, preferred_element_type=jnp.float32
    )
    count_second = jnp.dot(
        hot_second.astype(jnp.bfloat16), earlier, preferred_element_type=jnp.float32
    ) + jnp.sum(hot_first, axis=1, keepdims=True)
    rank_first = jnp.sum(count_first * hot_first, axis=0, keepdims=True).astype(jnp.int32)
    rank_second = jnp.sum(count_second * hot_second, axis=0, keepdims=True).astype(jnp.int32)
    row_first = first * 8 + rank_first
    row_second = second * 8 + rank_second
    slot_row = lax.broadcasted_iota(jnp.int32, (spread.shape[0], tokens), 0)
    for half in range(2):
        picked = (slot_row == row_first + 4 * half) | (slot_row == row_second + 4 * half)
        spread[:, half * 128 : half * 128 + 128] = picked.astype(jnp.float32).astype(jnp.bfloat16)
    wide = lane_iota(tokens, 512)

    def down(row):
        return jnp.broadcast_to(row.astype(jnp.float32), (tokens, tokens)).T[:, 0:1]

    for k, (chosen, rank) in enumerate(((first, rank_first), (second, rank_second))):
        target = down(chosen * SLOTS + rank).astype(jnp.int32)
        gather[k * tokens : (k + 1) * tokens, :] = (
            (target == wide).astype(jnp.float32).astype(jnp.bfloat16)
        )
    total = shares[0:1, :] + shares[1:2, :]
    weight[:, 0:1] = down(group_prob[...] * shares[0:1, :] / total)
    weight[:, 1:2] = down(group_prob[...] * shares[1:2, :] / total)


def start_moves(pairs, arrivals):
    moves = [
        pltpu.make_async_copy(source, target, arrivals.at[k])
        for k, (source, target) in enumerate(pairs)
    ]
    for move in moves:
        move.start()
    return moves


def pack_kernel(latent, rope, latent_gain, out, latent_here, rope_here, latent_gain_here, arrivals):
    moves = start_moves(
        ((latent_gain, latent_gain_here), (rope, rope_here), (latent, latent_here)), arrivals
    )
    for move in moves:
        move.wait()
    rows = latent_here.shape[0]
    raw = latent_here[...].astype(jnp.float32)
    normed = (raw * inverse_rms(raw, raw.shape[1]) * latent_gain_here[...]).astype(jnp.bfloat16)
    block = rows + 16
    first, second = rope_here[0:16, :], rope_here[16:32, :]
    for device in range(out.shape[0] // block):
        at = device * block
        out[at : at + rows, :] = normed
        out[at + rows : at + block, 0:128] = first
        out[at + rows : at + block, 128:256] = second


def query_kernel(
    query,
    query_gain,
    key_weight,
    cos_table,
    sin_table,
    choice,
    group_prob,
    shares,
    out,
    key_weight_turned,
    spread,
    gather,
    weight,
    query_here,
    query_gain_here,
    key_weight_here,
    arrivals,
    small,
    turn,
):
    moves = start_moves(
        (
            (query_gain, query_gain_here),
            (query, query_here),
            (key_weight, key_weight_here),
        ),
        arrivals,
    )
    route(choice, group_prob, shares, spread, gather, weight)
    query = query_here
    rows = query.shape[0]
    heads = query.shape[1] // 96
    lane = lane_iota(rows)
    early = lax.broadcasted_iota(jnp.int32, (rows, LANES), 0) < SPAN
    for move in moves:
        move.wait()
    key_weight_turned[...] = key_weight_here[...].astype(jnp.float32).T.astype(jnp.bfloat16)
    small[...] = jnp.zeros(small.shape, jnp.float32)
    small[0:1, 0:96] = query_gain_here[...]
    turn[:, 0:128] = jnp.ones((rows, 128), jnp.float32)
    turn[:, 128:384] = jnp.zeros((rows, 256), jnp.float32)
    turn[:, 64:80] = cos_table[...]
    turn[:, 80:96] = cos_table[...]
    turn[:, 192:208] = -sin_table[...]
    turn[:, 336:352] = sin_table[...]
    tables = [turn[:, 0:128], turn[:, 128:256], turn[:, 256:384]]
    gain_row = small[0:8, :]
    gain_tiles = [
        (gain_row + pltpu.roll(gain_row, 96, 1) * (lane_iota(8) >= 96).astype(jnp.float32))[0:1],
        jnp.where(lane_iota(8) < 64, pltpu.roll(gain_row, 96, 1), pltpu.roll(gain_row, 64, 1))[0:1],
        jnp.where(lane_iota(8) < 32, pltpu.roll(gain_row, 64, 1), pltpu.roll(gain_row, 32, 1))[0:1],
    ]
    turn_tiles = [
        tables,
        [pltpu.roll(t, 96, 1) for t in tables],
        [jnp.where(lane < 64, pltpu.roll(t, 64, 1), pltpu.roll(t, 32, 1)) for t in tables],
    ]
    wide_row = lax.broadcasted_iota(jnp.int32, (128, 256), 0)
    wide_lane = lax.broadcasted_iota(jnp.int32, (128, 256), 1)
    sum_low = same_group(wide_row // 96, wide_lane // 96)
    sum_mid = same_group((wide_row + 128) // 96, wide_lane // 96)
    sum_mid_last = same_group(
        (lax.broadcasted_iota(jnp.int32, (128, 128), 0) + 128) // 96, (lane_iota(128) + 256) // 96
    )
    sum_high = same_group((wide_row + 256) // 96, (wide_lane + 128) // 96)

    def masking(begin):
        return jnp.where(
            lane == begin, 1.0, jnp.where((lane == begin + 1) & early, 1.0, 0.0)
        )

    free = [lane >= 96, (lane >= 64) & (lane < 96), (lane >= 32) & (lane < 64), lane < 32]
    selects = [masking(begin) for begin in (96, 64, 32, 0)]
    for four in range(heads // 4):
        raw = [
            query[:, four * 384 + t * 128 : four * 384 + t * 128 + 128].astype(jnp.float32)
            for t in range(3)
        ]
        squares = [split_high_low(t * t) for t in raw]
        from_low = jnp.dot(squares[0], sum_low, preferred_element_type=jnp.float32)
        from_mid = jnp.dot(squares[1], sum_mid, preferred_element_type=jnp.float32)
        from_mid_last = jnp.dot(squares[1], sum_mid_last, preferred_element_type=jnp.float32)
        from_high = jnp.dot(squares[2], sum_high, preferred_element_type=jnp.float32)
        sums = [
            from_low[:, :128] + from_mid[:, :128],
            from_low[:, 128:] + from_mid[:, 128:] + from_high[:, :128],
            from_mid_last + from_high[:, 128:],
        ]
        turned = [
            turn_lanes(
                raw[t] * lax.rsqrt(sums[t] * (1.0 / 96) + eps) * gain_tiles[t], *turn_tiles[t]
            )
            for t in range(3)
        ]
        query_at = [
            turned[0],
            jnp.where(lane < 96, turned[1], turned[0]),
            jnp.where(lane < 64, turned[2], turned[1]),
            turned[2],
        ]
        for k in range(4):
            head = four * 4 + k
            out[head * rows : (head + 1) * rows, :] = jnp.where(
                free[k], selects[k], query_at[k]
            ).astype(jnp.bfloat16)


def attend_kernel(
    gathered,
    query,
    key_weight_turned,
    query_gain,
    key_gain,
    cos_all,
    sin_all,
    value_weight_far,
    out_weight,
    out,
    out_weight_here,
    value_weight,
    latents,
    key_parts,
    keys,
    ropes,
    sums,
    weights,
    arrivals,
):
    moves = start_moves(
        ((value_weight_far, value_weight), (out_weight, out_weight_here)), arrivals
    )
    own = lax.axis_index("sp")
    tokens = query.shape[0] // 16
    block = tokens + 16
    length = latents.shape[0]
    heads = key_weight_turned.shape[0] // 64
    scale = 96 ** (-0.5) * 1.4426950408889634
    half_gain = [key_gain[64:80, 0:1], key_gain[80:96, 0:1]]
    for device in range(length // tokens):
        at, here = device * block, slice(device * tokens, (device + 1) * tokens)
        latents[here, :] = gathered[at : at + tokens, :]
        first = gathered[at + tokens : at + block, 0:128].astype(jnp.float32)
        second = gathered[at + tokens : at + block, 128:256].astype(jnp.float32)
        sums[:, here] = jnp.sum(first * first + second * second, axis=0, keepdims=True)
        first, second = first * half_gain[0], second * half_gain[1]
        cos_part, sin_part = cos_all[:, here], sin_all[:, here]
        ropes[0:16, here] = first * cos_part - second * sin_part
        ropes[16:32, here] = second * cos_part + first * sin_part
    row = lax.broadcasted_iota(jnp.int32, (32, length), 0)
    key = lax.broadcasted_iota(jnp.int32, (32, length), 1)
    later = (row == 0) & (key >= (own + 1) * tokens)
    beside = (row == 1) & (key >= own * tokens + SPAN) & (key < (own + 1) * tokens)
    hidden = jnp.where(later | beside, -1e30, 0.0).astype(jnp.bfloat16)
    for k in range(4):
        keys[k, (96 * k + 96) % 128 : (96 * k + 96) % 128 + 32, :] = hidden
    for at in range(0, length, 256):
        key_parts[:, at : at + 256] = lax.dot_general(
            key_weight_turned[...],
            latents[at : at + 256, :],
            (((1,), (1,)), ((), ())),
            preferred_element_type=jnp.float32,
        ).astype(jnp.bfloat16)
    low_gain = jnp.broadcast_to(key_gain[0:64, 0:1], (64, 128))
    low_gain = jnp.concatenate([low_gain] * (length // 128), axis=1)

    def scores_of(head, kind):
        part = key_parts[pl.ds(head * 64, 64), :].astype(jnp.float32)
        total = jnp.sum(part * part, axis=0, keepdims=True) + sums[...]
        inverse = lax.rsqrt(total * (1.0 / 96) + eps)
        part = (part * inverse * low_gain).astype(jnp.bfloat16)
        turned = (ropes[...] * inverse).astype(jnp.bfloat16)
        begin = (96 * kind) % 128
        for piece, source in ((0, part[0:32]), (32, part[32:64]), (64, turned)):
            at = (begin + piece) % 128
            keys[kind, at : at + 32, :] = source
        return jnp.dot(
            query[pl.ds(head * tokens, tokens), :],
            keys[kind],
            preferred_element_type=jnp.float32,
        )

    def fold(array, combine):
        parts = [array[:, at : at + 128] for at in range(0, array.shape[1], 128)]
        while len(parts) > 1:
            parts = [combine(*parts[at : at + 2]) for at in range(0, len(parts), 2)]
        return parts[0]

    lane = lane_iota(tokens)

    def finish(first_head, count, buffer, row_sums):
        mixed = jnp.dot(
            weights[buffer, 0 : count * tokens, :], latents[...], preferred_element_type=jnp.float32
        )
        for two in range(0, count, 2):
            rows = [
                mixed[(two + odd) * tokens : (two + odd + 1) * tokens] * (1.0 / row_sums[two + odd])
                for odd in range(2)
            ]
            at = first_head * 64 + two * 64
            at = at if isinstance(at, int) else pl.multiple_of(at, 128)
            both = jnp.dot(
                jnp.concatenate(rows, axis=0).astype(jnp.bfloat16),
                value_weight[:, pl.ds(at, 128)],
                preferred_element_type=jnp.float32,
            )
            out[:, pl.ds(at, 128)] = jnp.where(lane < 64, both[:tokens], both[tokens:]).astype(
                jnp.bfloat16
            )

    moves[0].wait()
    bound = 14.2 * jnp.max(jnp.abs(query_gain[...])) * jnp.max(jnp.abs(key_gain[...]))
    narrow = bound < 100.0

    @pl.when(narrow)
    def _():
        waiting = None
        for first_head in range(0, heads, 2):
            buffer = (first_head // 2) % 2
            row_sums = []
            for k in range(2):
                raised = jnp.exp2(scores_of(first_head + k, (first_head + k) % 4) * scale)
                row_sums.append(jnp.sum(fold(raised, jnp.add), axis=-1, keepdims=True))
                weights[buffer, k * tokens : (k + 1) * tokens, :] = raised.astype(jnp.bfloat16)
            if waiting is not None:
                finish(*waiting)
            waiting = (first_head, 2, buffer, row_sums)
        finish(*waiting)

    @pl.when(jnp.logical_not(narrow))
    def _():
        def four_heads(step, carry):
            row_sums = []
            for kind in range(4):
                scores = scores_of(step * 4 + kind, kind)
                top = jnp.max(fold(scores, jnp.maximum), axis=-1, keepdims=True)
                raised = jnp.exp2((scores - top) * scale)
                row_sums.append(jnp.sum(fold(raised, jnp.add), axis=-1, keepdims=True))
                at = (kind % 2) * tokens
                weights[kind // 2, at : at + tokens, :] = raised.astype(jnp.bfloat16)
                if kind % 2:
                    finish(step * 4 + kind - 1, 2, kind // 2, row_sums[kind - 1 :])
            return carry

        lax.fori_loop(0, heads // 4, four_heads, 0)

    moves[1].wait()


def mix_kernel(heads_out, residual, mix_gain, out_weight, ffn_gain, spread, stream_out, outgoing):
    width = residual.shape[1]
    wide = heads_out[...].astype(jnp.float32)
    mixed_in = (wide * inverse_rms(wide, wide.shape[1]) * mix_gain[...]).astype(jnp.bfloat16)
    stream = residual[...].astype(jnp.float32) + jnp.dot(
        mixed_in, out_weight[...], preferred_element_type=jnp.float32
    )
    stream_out[...] = stream
    normed = (stream * inverse_rms(stream, width) * ffn_gain[...]).astype(jnp.bfloat16)
    stacked = jnp.concatenate([normed[:, : width // 2], normed[:, width // 2 :]], axis=0)
    outgoing[...] = jnp.dot(
        spread[...], stacked, preferred_element_type=jnp.float32
    ).astype(jnp.bfloat16)


def unstack(blocks, rows_out):
    pairs, width = blocks.shape[0] // 16, blocks.shape[1]
    view = blocks[...].astype(jnp.float32).reshape(pairs, 2, 8, width)
    one, two = view[:, 0], view[:, 1]
    upper = lax.broadcasted_iota(jnp.int32, (pairs, 8, width), 1) < 4
    low = jnp.where(upper, one, pltpu.roll(two, 4, 1))
    high = jnp.where(upper, pltpu.roll(one, 4, 1), two)
    rows_out[:, 0:width] = low.reshape(pairs * 8, width).astype(jnp.bfloat16)
    rows_out[:, width : 2 * width] = high.reshape(pairs * 8, width).astype(jnp.bfloat16)


def expert_kernel(arrived, gate_weight, up_weight, down_weight, out, rows_in):
    unstack(arrived, rows_in)
    gate_act = jnp.dot(rows_in[...], gate_weight[0], preferred_element_type=jnp.float32)
    upward = jnp.dot(rows_in[...], up_weight[0], preferred_element_type=jnp.float32)
    hidden = (jax.nn.silu(gate_act) * upward).astype(jnp.bfloat16)
    expert_out = jnp.dot(hidden, down_weight[0], preferred_element_type=jnp.float32)
    rows, width = expert_out.shape
    width = width // 2
    low = expert_out[:, :width].reshape(rows // 8, 8, width)
    high = expert_out[:, width:].reshape(rows // 8, 8, width)
    upper = lax.broadcasted_iota(jnp.int32, (rows // 8, 8, width), 1) < 4
    one = jnp.where(upper, low, pltpu.roll(high, 4, 1))
    two = jnp.where(upper, pltpu.roll(low, 4, 1), high)
    both = jnp.concatenate([one[:, None], two[:, None]], axis=1)
    out[...] = both.reshape(rows * 2, width).astype(jnp.bfloat16)


def combine_kernel(returned, gather, stream, route_weight, out, rows_back):
    unstack(returned, rows_back)
    tokens = stream.shape[0]
    picked = jnp.dot(gather[...], rows_back[...], preferred_element_type=jnp.float32)
    routed = route_weight[:, 0:1] * picked[:tokens] + route_weight[:, 1:2] * picked[tokens:]
    out[...] = (stream[...] + routed).astype(jnp.bfloat16)


VMEM = pl.BlockSpec(memory_space=pltpu.VMEM)
HBM = pl.BlockSpec(memory_space=pltpu.HBM)


def call(body, in_specs, out_shapes, mib, scratch=(), name=None):
    many = isinstance(out_shapes, tuple)
    run = pl.pallas_call(
        body,
        in_specs=in_specs,
        out_shape=out_shapes,
        out_specs=tuple(VMEM for _ in out_shapes) if many else VMEM,
        scratch_shapes=list(scratch),
        compiler_params=pltpu.CompilerParams(vmem_limit_bytes=mib * 2**20),
        name=name,
    )

    def placed(*operands):
        return run(
            *(
                pltpu.with_memory_space_constraint(x, pltpu.HBM) if spec is HBM else x
                for spec, x in zip(in_specs, operands)
            )
        )

    return placed


def per_device(
    residual,
    query,
    latent,
    rope_key,
    latent_gain,
    query_gain,
    key_gain,
    key_weight,
    value_weight,
    mix_gain,
    out_weight,
    ffn_gain,
    expert_choice,
    group_prob,
    expert_prob,
    gate_weight,
    up_weight,
    down_weight,
):
    tokens = residual.shape[1]
    width = residual.shape[2]
    devices = lax.axis_size("sp")
    sequence = tokens * devices
    shape = jax.ShapeDtypeStruct
    half, full = jnp.bfloat16, jnp.float32
    block = tokens + 16
    packed = call(
        pack_kernel,
        [HBM] * 3,
        shape((devices * block, 256), half),
        6,
        scratch=(
            pltpu.VMEM(latent.shape[1:], half),
            pltpu.VMEM(rope_key.shape[:0:-1], half),
            pltpu.VMEM((1,) + latent_gain.shape, full),
            pltpu.SemaphoreType.DMA((3,)),
        ),
        name="pack",
    )(latent[0], rope_key[0].T, latent_gain[None])
    gathered = lax.all_to_all(packed, "sp", split_axis=0, concat_axis=0, tiled=True)
    own = angles(lax.axis_index("sp") * tokens, tokens, rope_key.shape[2])
    every = angles(0, sequence, rope_key.shape[2]).T
    (
        queries,
        key_weight_turned,
        spread,
        gather,
        route_weight,
    ) = call(
        query_kernel,
        [HBM] * 3 + [VMEM] * 5,
        (
            shape((16 * tokens, 128), half),
            shape(key_weight.shape[::-1], half),
            shape((1024, 256), half),
            shape((256, 512), half),
            shape((tokens, 2), full),
        ),
        22,
        scratch=(
            pltpu.VMEM(query.shape[1:], half),
            pltpu.VMEM((1,) + query_gain.shape, full),
            pltpu.VMEM(key_weight.shape, half),
            pltpu.SemaphoreType.DMA((3,)),
            pltpu.VMEM((8, 128), full),
            pltpu.VMEM((tokens, 384), full),
        ),
        name="query",
    )(
        query[0],
        query_gain[None],
        key_weight,
        jnp.cos(own),
        jnp.sin(own),
        expert_choice[0].T,
        group_prob,
        expert_prob[0].T,
    )
    heads_out, out_weight = call(
        attend_kernel,
        [VMEM] * 7 + [HBM] * 2,
        (shape((tokens, 1024), half), shape(out_weight.shape, half)),
        30,
        scratch=(
            pltpu.VMEM(value_weight.shape, half),
            pltpu.VMEM((sequence, 256), half),
            pltpu.VMEM((1024, sequence), half),
            pltpu.VMEM((4, 128, sequence), half),
            pltpu.VMEM((32, sequence), full),
            pltpu.VMEM((1, sequence), full),
            pltpu.VMEM((2, 2 * tokens, sequence), half),
            pltpu.SemaphoreType.DMA((2,)),
        ),
        name="attend",
    )(
        gathered,
        queries,
        key_weight_turned,
        query_gain[None],
        key_gain[:, None],
        jnp.cos(every),
        jnp.sin(every),
        value_weight,
        out_weight,
    )
    stream, outgoing = call(
        mix_kernel,
        [VMEM] * 6,
        (shape((tokens, width), full), shape((1024, 1024), half)),
        16,
        name="mix",
    )(heads_out, residual[0], mix_gain[None], out_weight, ffn_gain[None], spread)
    arrived = lax.all_to_all(outgoing, ("sp", "dp"), split_axis=0, concat_axis=0, tiled=True)
    answers = call(
        expert_kernel,
        [VMEM] * 4,
        shape((1024, 1024), half),
        20,
        scratch=(pltpu.VMEM((512, width), half),),
        name="expert",
    )(arrived, gate_weight, up_weight, down_weight)
    returned = lax.all_to_all(answers, ("sp", "dp"), split_axis=0, concat_axis=0, tiled=True)
    return call(
        combine_kernel,
        [VMEM] * 4,
        shape((tokens, width), half),
        14,
        scratch=(pltpu.VMEM((512, width), half),),
        name="combine",
    )(returned, gather, stream, route_weight)[None]


def solution(mesh):
    return jax.shard_map(
        per_device,
        mesh=mesh,
        in_specs=(
            P("dp", "sp", None),
            P("dp", "sp", None),
            P("dp", "sp", None),
            P("dp", "sp", None),
            P(),
            P(),
            P(),
            P(),
            P(),
            P(),
            P(),
            P(),
            P("dp", "sp", None),
            P("dp", "sp"),
            P("dp", "sp", None),
            P(("sp", "dp"), None, None),
            P(("sp", "dp"), None, None),
            P(("sp", "dp"), None, None),
        ),
        out_specs=P("dp", "sp", None),
        check_vma=False,
    )
```

```python
import jax
import jax.numpy as jnp
from jax import lax
from jax.experimental import pallas as pl
from jax.experimental.pallas import tpu as pltpu
from jax.sharding import PartitionSpec as P

SPAN = 64
LANES = 128
SLOTS = 4

eps = 1e-06


def angles(offset, span_count, rope_width):
    position = (offset + jnp.arange(span_count, dtype=jnp.int32)).astype(jnp.float32)
    frequency = 10000.0 ** (-2.0 * jnp.arange(rope_width // 2, dtype=jnp.float32) / rope_width)
    return position[:, None] * frequency[None, :]


def lane_iota(rows, width=LANES):
    return lax.broadcasted_iota(jnp.int32, (rows, width), 1)


def inverse_rms(vector, width):
    return lax.rsqrt(jnp.sum(vector * vector, axis=-1, keepdims=True) * (1.0 / width) + eps)


def turn_lanes(vector, cos_part, minus_sin, plus_sin):
    return (
        vector * cos_part
        + pltpu.roll(vector, 112, 1) * minus_sin
        + pltpu.roll(vector, 16, 1) * plus_sin
    )


def split_high_low(vector):
    high = vector.astype(jnp.bfloat16)
    low = (vector - high.astype(jnp.float32)).astype(jnp.bfloat16)
    return jnp.concatenate([high, low], axis=1)


def same_group(group_of_row, group_of_lane):
    ones = (group_of_row == group_of_lane).astype(jnp.float32).astype(jnp.bfloat16)
    return jnp.concatenate([ones, ones], axis=0)


def route(choice, group_prob, shares, spread, gather, weight):
    tokens = choice.shape[1]
    expert = lax.broadcasted_iota(jnp.int32, (LANES, tokens), 0)
    first = choice[0:1, :]
    second = choice[1:2, :]
    hot_first = (expert == first).astype(jnp.float32)
    hot_second = (expert == second).astype(jnp.float32)
    earlier = (
        (lax.broadcasted_iota(jnp.int32, (tokens, tokens), 0) < lane_iota(tokens, tokens))
        .astype(jnp.float32)
        .astype(jnp.bfloat16)
    )
    count_first = jnp.dot(
        hot_first.astype(jnp.bfloat16), earlier, preferred_element_type=jnp.float32
    )
    count_second = jnp.dot(
        hot_second.astype(jnp.bfloat16), earlier, preferred_element_type=jnp.float32
    ) + jnp.sum(hot_first, axis=1, keepdims=True)
    rank_first = jnp.sum(count_first * hot_first, axis=0, keepdims=True).astype(jnp.int32)
    rank_second = jnp.sum(count_second * hot_second, axis=0, keepdims=True).astype(jnp.int32)
    row_first = first * 8 + rank_first
    row_second = second * 8 + rank_second
    slot_row = lax.broadcasted_iota(jnp.int32, (spread.shape[0], tokens), 0)
    for half in range(2):
        picked = (slot_row == row_first + 4 * half) | (slot_row == row_second + 4 * half)
        spread[:, half * 128 : half * 128 + 128] = picked.astype(jnp.float32).astype(jnp.bfloat16)
    wide = lane_iota(tokens, 512)

    def down(row):
        return jnp.broadcast_to(row.astype(jnp.float32), (tokens, tokens)).T[:, 0:1]

    for k, (chosen, rank) in enumerate(((first, rank_first), (second, rank_second))):
        target = down(chosen * SLOTS + rank).astype(jnp.int32)
        gather[k * tokens : (k + 1) * tokens, :] = (
            (target == wide).astype(jnp.float32).astype(jnp.bfloat16)
        )
    total = shares[0:1, :] + shares[1:2, :]
    weight[:, 0:1] = down(group_prob[...] * shares[0:1, :] / total)
    weight[:, 1:2] = down(group_prob[...] * shares[1:2, :] / total)


def start_moves(pairs, arrivals):
    moves = [
        pltpu.make_async_copy(source, target, arrivals.at[k])
        for k, (source, target) in enumerate(pairs)
    ]
    for move in moves:
        move.start()
    return moves


def pack_kernel(latent, rope, latent_gain, out, latent_here, rope_here, latent_gain_here, arrivals):
    moves = start_moves(
        ((latent_gain, latent_gain_here), (rope, rope_here), (latent, latent_here)), arrivals
    )
    for move in moves:
        move.wait()
    rows = latent_here.shape[0]
    raw = latent_here[...].astype(jnp.float32)
    normed = (raw * inverse_rms(raw, raw.shape[1]) * latent_gain_here[...]).astype(jnp.bfloat16)
    block = rows + 16
    first, second = rope_here[0:16, :], rope_here[16:32, :]
    for device in range(out.shape[0] // block):
        at = device * block
        out[at : at + rows, :] = normed
        out[at + rows : at + block, 0:128] = first
        out[at + rows : at + block, 128:256] = second


def query_kernel(
    query,
    query_gain,
    key_weight,
    cos_table,
    sin_table,
    choice,
    group_prob,
    shares,
    out,
    key_weight_turned,
    spread,
    gather,
    weight,
    query_here,
    query_gain_here,
    key_weight_here,
    arrivals,
    small,
    turn,
):
    moves = start_moves(
        (
            (query_gain, query_gain_here),
            (query, query_here),
            (key_weight, key_weight_here),
        ),
        arrivals,
    )
    route(choice, group_prob, shares, spread, gather, weight)
    query = query_here
    rows = query.shape[0]
    heads = query.shape[1] // 96
    lane = lane_iota(rows)
    early = lax.broadcasted_iota(jnp.int32, (rows, LANES), 0) < SPAN
    for move in moves:
        move.wait()
    key_weight_turned[...] = key_weight_here[...].astype(jnp.float32).T.astype(jnp.bfloat16)
    small[...] = jnp.zeros(small.shape, jnp.float32)
    small[0:1, 0:96] = query_gain_here[...]
    turn[:, 0:128] = jnp.ones((rows, 128), jnp.float32)
    turn[:, 128:384] = jnp.zeros((rows, 256), jnp.float32)
    turn[:, 64:80] = cos_table[...]
    turn[:, 80:96] = cos_table[...]
    turn[:, 192:208] = -sin_table[...]
    turn[:, 336:352] = sin_table[...]
    tables = [turn[:, 0:128], turn[:, 128:256], turn[:, 256:384]]
    gain_row = small[0:8, :]
    gain_tiles = [
        (gain_row + pltpu.roll(gain_row, 96, 1) * (lane_iota(8) >= 96).astype(jnp.float32))[0:1],
        jnp.where(lane_iota(8) < 64, pltpu.roll(gain_row, 96, 1), pltpu.roll(gain_row, 64, 1))[0:1],
        jnp.where(lane_iota(8) < 32, pltpu.roll(gain_row, 64, 1), pltpu.roll(gain_row, 32, 1))[0:1],
    ]
    turn_tiles = [
        tables,
        [pltpu.roll(t, 96, 1) for t in tables],
        [jnp.where(lane < 64, pltpu.roll(t, 64, 1), pltpu.roll(t, 32, 1)) for t in tables],
    ]
    wide_row = lax.broadcasted_iota(jnp.int32, (128, 256), 0)
    wide_lane = lax.broadcasted_iota(jnp.int32, (128, 256), 1)
    sum_low = same_group(wide_row // 96, wide_lane // 96)
    sum_mid = same_group((wide_row + 128) // 96, wide_lane // 96)
    sum_mid_last = same_group(
        (lax.broadcasted_iota(jnp.int32, (128, 128), 0) + 128) // 96, (lane_iota(128) + 256) // 96
    )
    sum_high = same_group((wide_row + 256) // 96, (wide_lane + 128) // 96)

    def masking(begin):
        return jnp.where(
            lane == begin, 1.0, jnp.where((lane == begin + 1) & early, 1.0, 0.0)
        )

    free = [lane >= 96, (lane >= 64) & (lane < 96), (lane >= 32) & (lane < 64), lane < 32]
    selects = [masking(begin) for begin in (96, 64, 32, 0)]
    for four in range(heads // 4):
        raw = [
            query[:, four * 384 + t * 128 : four * 384 + t * 128 + 128].astype(jnp.float32)
            for t in range(3)
        ]
        squares = [split_high_low(t * t) for t in raw]
        from_low = jnp.dot(squares[0], sum_low, preferred_element_type=jnp.float32)
        from_mid = jnp.dot(squares[1], sum_mid, preferred_element_type=jnp.float32)
        from_mid_last = jnp.dot(squares[1], sum_mid_last, preferred_element_type=jnp.float32)
        from_high = jnp.dot(squares[2], sum_high, preferred_element_type=jnp.float32)
        sums = [
            from_low[:, :128] + from_mid[:, :128],
            from_low[:, 128:] + from_mid[:, 128:] + from_high[:, :128],
            from_mid_last + from_high[:, 128:],
        ]
        turned = [
            turn_lanes(
                raw[t] * lax.rsqrt(sums[t] * (1.0 / 96) + eps) * gain_tiles[t], *turn_tiles[t]
            )
            for t in range(3)
        ]
        query_at = [
            turned[0],
            jnp.where(lane < 96, turned[1], turned[0]),
            jnp.where(lane < 64, turned[2], turned[1]),
            turned[2],
        ]
        for k in range(4):
            head = four * 4 + k
            out[head * rows : (head + 1) * rows, :] = jnp.where(
                free[k], selects[k], query_at[k]
            ).astype(jnp.bfloat16)


def attend_kernel(
    gathered,
    query,
    key_weight_turned,
    query_gain,
    key_gain,
    cos_all,
    sin_all,
    value_weight_far,
    out_weight,
    out,
    out_weight_here,
    value_weight,
    latents,
    key_parts,
    keys,
    ropes,
    sums,
    weights,
    arrivals,
):
    moves = start_moves(
        ((value_weight_far, value_weight), (out_weight, out_weight_here)), arrivals
    )
    own = lax.axis_index("sp")
    tokens = query.shape[0] // 16
    block = tokens + 16
    length = latents.shape[0]
    heads = key_weight_turned.shape[0] // 64
    scale = 96 ** (-0.5) * 1.4426950408889634
    half_gain = [key_gain[64:80, 0:1], key_gain[80:96, 0:1]]
    for device in range(length // tokens):
        at, here = device * block, slice(device * tokens, (device + 1) * tokens)
        latents[here, :] = gathered[at : at + tokens, :]
        first = gathered[at + tokens : at + block, 0:128].astype(jnp.float32)
        second = gathered[at + tokens : at + block, 128:256].astype(jnp.float32)
        sums[:, here] = jnp.sum(first * first + second * second, axis=0, keepdims=True)
        first, second = first * half_gain[0], second * half_gain[1]
        cos_part, sin_part = cos_all[:, here], sin_all[:, here]
        ropes[0:16, here] = first * cos_part - second * sin_part
        ropes[16:32, here] = second * cos_part + first * sin_part
    row = lax.broadcasted_iota(jnp.int32, (32, length), 0)
    key = lax.broadcasted_iota(jnp.int32, (32, length), 1)
    later = (row == 0) & (key >= (own + 1) * tokens)
    beside = (row == 1) & (key >= own * tokens + SPAN) & (key < (own + 1) * tokens)
    hidden = jnp.where(later | beside, -1e30, 0.0).astype(jnp.bfloat16)
    for k in range(4):
        keys[k, (96 * k + 96) % 128 : (96 * k + 96) % 128 + 32, :] = hidden
    for at in range(0, length, 256):
        key_parts[:, at : at + 256] = lax.dot_general(
            key_weight_turned[...],
            latents[at : at + 256, :],
            (((1,), (1,)), ((), ())),
            preferred_element_type=jnp.float32,
        ).astype(jnp.bfloat16)
    low_gain = jnp.broadcast_to(key_gain[0:64, 0:1], (64, 128))
    low_gain = jnp.concatenate([low_gain] * (length // 128), axis=1)

    def scores_of(head, kind):
        part = key_parts[pl.ds(head * 64, 64), :].astype(jnp.float32)
        total = jnp.sum(part * part, axis=0, keepdims=True) + sums[...]
        inverse = lax.rsqrt(total * (1.0 / 96) + eps)
        part = (part * inverse * low_gain).astype(jnp.bfloat16)
        turned = (ropes[...] * inverse).astype(jnp.bfloat16)
        begin = (96 * kind) % 128
        for piece, source in ((0, part[0:32]), (32, part[32:64]), (64, turned)):
            at = (begin + piece) % 128
            keys[kind, at : at + 32, :] = source
        return jnp.dot(
            query[pl.ds(head * tokens, tokens), :],
            keys[kind],
            preferred_element_type=jnp.float32,
        )

    def fold(array, combine):
        parts = [array[:, at : at + 128] for at in range(0, array.shape[1], 128)]
        while len(parts) > 1:
            parts = [combine(*parts[at : at + 2]) for at in range(0, len(parts), 2)]
        return parts[0]

    lane = lane_iota(tokens)

    def finish(first_head, count, buffer, row_sums):
        mixed = jnp.dot(
            weights[buffer, 0 : count * tokens, :], latents[...], preferred_element_type=jnp.float32
        )
        for two in range(0, count, 2):
            rows = [
                mixed[(two + odd) * tokens : (two + odd + 1) * tokens] * (1.0 / row_sums[two + odd])
                for odd in range(2)
            ]
            at = first_head * 64 + two * 64
            at = at if isinstance(at, int) else pl.multiple_of(at, 128)
            both = jnp.dot(
                jnp.concatenate(rows, axis=0).astype(jnp.bfloat16),
                value_weight[:, pl.ds(at, 128)],
                preferred_element_type=jnp.float32,
            )
            out[:, pl.ds(at, 128)] = jnp.where(lane < 64, both[:tokens], both[tokens:]).astype(
                jnp.bfloat16
            )

    moves[0].wait()
    bound = 14.2 * jnp.max(jnp.abs(query_gain[...])) * jnp.max(jnp.abs(key_gain[...]))
    narrow = bound < 100.0

    @pl.when(narrow)
    def _():
        waiting = None
        for first_head in range(0, heads, 2):
            buffer = (first_head // 2) % 2
            row_sums = []
            for k in range(2):
                raised = jnp.exp2(scores_of(first_head + k, (first_head + k) % 4) * scale)
                row_sums.append(jnp.sum(fold(raised, jnp.add), axis=-1, keepdims=True))
                weights[buffer, k * tokens : (k + 1) * tokens, :] = raised.astype(jnp.bfloat16)
            if waiting is not None:
                finish(*waiting)
            waiting = (first_head, 2, buffer, row_sums)
        finish(*waiting)

    @pl.when(jnp.logical_not(narrow))
    def _():
        def four_heads(step, carry):
            row_sums = []
            for kind in range(4):
                scores = scores_of(step * 4 + kind, kind)
                top = jnp.max(fold(scores, jnp.maximum), axis=-1, keepdims=True)
                raised = jnp.exp2((scores - top) * scale)
                row_sums.append(jnp.sum(fold(raised, jnp.add), axis=-1, keepdims=True))
                at = (kind % 2) * tokens
                weights[kind // 2, at : at + tokens, :] = raised.astype(jnp.bfloat16)
                if kind % 2:
                    finish(step * 4 + kind - 1, 2, kind // 2, row_sums[kind - 1 :])
            return carry

        lax.fori_loop(0, heads // 4, four_heads, 0)

    moves[1].wait()


def mix_kernel(heads_out, residual, mix_gain, out_weight, ffn_gain, spread, stream_out, outgoing):
    width = residual.shape[1]
    wide = heads_out[...].astype(jnp.float32)
    mixed_in = (wide * inverse_rms(wide, wide.shape[1]) * mix_gain[...]).astype(jnp.bfloat16)
    stream = residual[...].astype(jnp.float32) + jnp.dot(
        mixed_in, out_weight[...], preferred_element_type=jnp.float32
    )
    stream_out[...] = stream
    normed = (stream * inverse_rms(stream, width) * ffn_gain[...]).astype(jnp.bfloat16)
    stacked = jnp.concatenate([normed[:, : width // 2], normed[:, width // 2 :]], axis=0)
    outgoing[...] = jnp.dot(
        spread[...], stacked, preferred_element_type=jnp.float32
    ).astype(jnp.bfloat16)


def unstack(blocks, rows_out, lanes):
    pairs, width = blocks.shape[0] // 16, lanes.stop - lanes.start
    view = blocks[:, lanes].astype(jnp.float32).reshape(pairs, 2, 8, width)
    one, two = view[:, 0], view[:, 1]
    upper = lax.broadcasted_iota(jnp.int32, (pairs, 8, width), 1) < 4
    low = jnp.where(upper, one, pltpu.roll(two, 4, 1))
    high = jnp.where(upper, pltpu.roll(one, 4, 1), two)
    spans = [slice(lanes.start + at, lanes.stop + at) for at in (0, blocks.shape[1])]
    rows_out[:, spans[0]] = low.reshape(pairs * 8, width).astype(jnp.bfloat16)
    rows_out[:, spans[1]] = high.reshape(pairs * 8, width).astype(jnp.bfloat16)
    return spans


def expert_kernel(arrived, gate_weight, up_weight, down_weight, out, rows_in):
    unstack(arrived, rows_in, slice(0, arrived.shape[1]))
    gate_act = jnp.dot(rows_in[...], gate_weight[0], preferred_element_type=jnp.float32)
    upward = jnp.dot(rows_in[...], up_weight[0], preferred_element_type=jnp.float32)
    hidden = (jax.nn.silu(gate_act) * upward).astype(jnp.bfloat16)
    expert_out = jnp.dot(hidden, down_weight[0], preferred_element_type=jnp.float32)
    rows, width = expert_out.shape
    width = width // 2
    low = expert_out[:, :width].reshape(rows // 8, 8, width)
    high = expert_out[:, width:].reshape(rows // 8, 8, width)
    upper = lax.broadcasted_iota(jnp.int32, (rows // 8, 8, width), 1) < 4
    one = jnp.where(upper, low, pltpu.roll(high, 4, 1))
    two = jnp.where(upper, pltpu.roll(low, 4, 1), high)
    both = jnp.concatenate([one[:, None], two[:, None]], axis=1)
    out[...] = both.reshape(rows * 2, width).astype(jnp.bfloat16)


def combine_kernel(
    returned, gather, stream, route_weight, out, rows_back, result, departures
):
    tokens = stream.shape[0]
    moves = []
    for at in range(0, returned.shape[1], 512):
        for span in unstack(returned, rows_back, slice(at, at + 512)):
            picked = jnp.dot(gather[...], rows_back[:, span], preferred_element_type=jnp.float32)
            routed = route_weight[:, 0:1] * picked[:tokens] + route_weight[:, 1:2] * picked[tokens:]
            result[:, span] = (stream[:, span] + routed).astype(jnp.bfloat16)
            moves.append(
                pltpu.make_async_copy(
                    result.at[:, span], out.at[:, span], departures.at[len(moves)]
                )
            )
            moves[-1].start()
    for move in moves:
        move.wait()


VMEM = pl.BlockSpec(memory_space=pltpu.VMEM)
HBM = pl.BlockSpec(memory_space=pltpu.HBM)


def call(body, in_specs, out_shapes, mib, scratch=(), name=None, out_spec=VMEM):
    many = isinstance(out_shapes, tuple)
    run = pl.pallas_call(
        body,
        in_specs=in_specs,
        out_shape=out_shapes,
        out_specs=tuple(out_spec for _ in out_shapes) if many else out_spec,
        scratch_shapes=list(scratch),
        compiler_params=pltpu.CompilerParams(vmem_limit_bytes=mib * 2**20),
        name=name,
    )

    def placed(*operands):
        return run(
            *(
                pltpu.with_memory_space_constraint(x, pltpu.HBM) if spec is HBM else x
                for spec, x in zip(in_specs, operands)
            )
        )

    return placed


def per_device(
    residual,
    query,
    latent,
    rope_key,
    latent_gain,
    query_gain,
    key_gain,
    key_weight,
    value_weight,
    mix_gain,
    out_weight,
    ffn_gain,
    expert_choice,
    group_prob,
    expert_prob,
    gate_weight,
    up_weight,
    down_weight,
):
    tokens = residual.shape[1]
    width = residual.shape[2]
    devices = lax.axis_size("sp")
    sequence = tokens * devices
    shape = jax.ShapeDtypeStruct
    half, full = jnp.bfloat16, jnp.float32
    block = tokens + 16
    packed = call(
        pack_kernel,
        [HBM] * 3,
        shape((devices * block, 256), half),
        6,
        scratch=(
            pltpu.VMEM(latent.shape[1:], half),
            pltpu.VMEM(rope_key.shape[:0:-1], half),
            pltpu.VMEM((1,) + latent_gain.shape, full),
            pltpu.SemaphoreType.DMA((3,)),
        ),
        name="pack",
    )(latent[0], rope_key[0].T, latent_gain[None])
    gathered = lax.all_to_all(packed, "sp", split_axis=0, concat_axis=0, tiled=True)
    own = angles(lax.axis_index("sp") * tokens, tokens, rope_key.shape[2])
    every = angles(0, sequence, rope_key.shape[2]).T
    (
        queries,
        key_weight_turned,
        spread,
        gather,
        route_weight,
    ) = call(
        query_kernel,
        [HBM] * 3 + [VMEM] * 5,
        (
            shape((16 * tokens, 128), half),
            shape(key_weight.shape[::-1], half),
            shape((1024, 256), half),
            shape((256, 512), half),
            shape((tokens, 2), full),
        ),
        22,
        scratch=(
            pltpu.VMEM(query.shape[1:], half),
            pltpu.VMEM((1,) + query_gain.shape, full),
            pltpu.VMEM(key_weight.shape, half),
            pltpu.SemaphoreType.DMA((3,)),
            pltpu.VMEM((8, 128), full),
            pltpu.VMEM((tokens, 384), full),
        ),
        name="query",
    )(
        query[0],
        query_gain[None],
        key_weight,
        jnp.cos(own),
        jnp.sin(own),
        expert_choice[0].T,
        group_prob,
        expert_prob[0].T,
    )
    heads_out, out_weight = call(
        attend_kernel,
        [VMEM] * 7 + [HBM] * 2,
        (shape((tokens, 1024), half), shape(out_weight.shape, half)),
        30,
        scratch=(
            pltpu.VMEM(value_weight.shape, half),
            pltpu.VMEM((sequence, 256), half),
            pltpu.VMEM((1024, sequence), half),
            pltpu.VMEM((4, 128, sequence), half),
            pltpu.VMEM((32, sequence), full),
            pltpu.VMEM((1, sequence), full),
            pltpu.VMEM((2, 2 * tokens, sequence), half),
            pltpu.SemaphoreType.DMA((2,)),
        ),
        name="attend",
    )(
        gathered,
        queries,
        key_weight_turned,
        query_gain[None],
        key_gain[:, None],
        jnp.cos(every),
        jnp.sin(every),
        value_weight,
        out_weight,
    )
    stream, outgoing = call(
        mix_kernel,
        [VMEM] * 6,
        (shape((tokens, width), full), shape((1024, 1024), half)),
        16,
        name="mix",
    )(heads_out, residual[0], mix_gain[None], out_weight, ffn_gain[None], spread)
    arrived = lax.all_to_all(outgoing, ("sp", "dp"), split_axis=0, concat_axis=0, tiled=True)
    answers = call(
        expert_kernel,
        [VMEM] * 4,
        shape((1024, 1024), half),
        20,
        scratch=(pltpu.VMEM((512, width), half),),
        name="expert",
    )(arrived, gate_weight, up_weight, down_weight)
    returned = lax.all_to_all(answers, ("sp", "dp"), split_axis=0, concat_axis=0, tiled=True)
    return call(
        combine_kernel,
        [VMEM] * 4,
        shape((tokens, width), half),
        14,
        scratch=(
            pltpu.VMEM((512, width), half),
            pltpu.VMEM((tokens, width), half),
            pltpu.SemaphoreType.DMA((4,)),
        ),
        name="combine",
        out_spec=HBM,
    )(returned, gather, stream, route_weight)[None]


def solution(mesh):
    return jax.shard_map(
        per_device,
        mesh=mesh,
        in_specs=(
            P("dp", "sp", None),
            P("dp", "sp", None),
            P("dp", "sp", None),
            P("dp", "sp", None),
            P(),
            P(),
            P(),
            P(),
            P(),
            P(),
            P(),
            P(),
            P("dp", "sp", None),
            P("dp", "sp"),
            P("dp", "sp", None),
            P(("sp", "dp"), None, None),
            P(("sp", "dp"), None, None),
            P(("sp", "dp"), None, None),
        ),
        out_specs=P("dp", "sp", None),
        check_vma=False,
    )
```
